768 devices in a mesh: ep: 24 (over z, core), tp: 32 (over y, x).
Axes of the slice: x: 4, y: 8, z: 12, core: 2. Of those that a mesh axis runs over, the one named last changes fastest.
Arguments:
- tokens: bfloat16 [6144, 2048], P('ep'), may hold values from -6 to 6
- norm_gain: float32 [2048], replicated, may hold values from 0.1 to 1.9
- expert_ids: int32 [6144, 2], P('ep'), may hold values from 0 to 23, all different within a row; in each aligned block of 256 rows (0 to 255, 256 to 511, ...) at most 32 rows name the same one
- routing_weight: float32 [6144, 2], P('ep'), may hold values from 0.1 to 1
- expert_gate: bfloat16 [24, 2048, 5632], P('ep', None, 'tp'), may hold values from -0.125 to 0.125
- expert_up: bfloat16 [24, 2048, 5632], P('ep', None, 'tp'), may hold values from -0.125 to 0.125
- expert_down: bfloat16 [24, 5632, 2048], P('ep', 'tp'), may hold values from -0.078125 to 0.078125
- dense_gate_w: bfloat16 [2048, 1024], P(None, 'tp'), may hold values from -0.125 to 0.125
- dense_up_w: bfloat16 [2048, 1024], P(None, 'tp'), may hold values from -0.125 to 0.125
- dense_down_w: bfloat16 [1024, 2048], P('tp'), may hold values from -0.1875 to 0.1875
- dense_gate: float32 [2048], P('tp'), may hold values from -3 to 3
Outputs:
- layer_out: bfloat16 [6144, 2048], P('ep', 'tp')
The draws below stay inside these ranges and needn't reach their ends.
Inputs may be any that keep to these rules, and one draw needn't show every extreme that they name: `expert_ids`: within the 256 rows of one device along ep, each row names two different experts and no expert is named by more than 32 rows; some expert is named by exactly 32 rows.
All inputs are finite; a program needn't handle non-finite values.
Results may differ from the reference program's by a relative error of at most 0.017.
Values may be sent and summed in bfloat16 or wider, within the bound.
No kernel may reach another device: no remote copies, remote signals or barrier semaphores. Data moves between devices by JAX's collectives and lax.ppermute only.
A program may use at most 64 MiB of HBM per device.

```python
import math
import jax
import jax.numpy as jnp
import numpy as np
from jax import lax

D = 2048
FF = 5632
DS = 1024
TOK_G = 256
EXPERTS = 24
CAP = 32
TOKENS = 6144
FF_PART = 176
DS_PART = 32
N_EP = 24
N_TP = 32


def block_levels(stream_key, dims, cuts, least, high):
    loudness, own = 1.0, jax.random.fold_in(stream_key, 6)
    for position, parts in cuts:
        steps = jnp.exp(jax.random.uniform(jax.random.fold_in(own, position), (parts,), jnp.float32, least / len(cuts), high / len(cuts)))
        loudness = loudness * jnp.repeat(steps, dims[position] // parts).reshape([-1 if axis == position else 1 for axis in range(len(dims))])
    return loudness


def shared_out(stream_key, own, number, rows, number_of, top, most, slope):
    order = jax.random.permutation(stream_key, number_of)
    packed, usual = portions_of(number_of, rows * top, most, slope, True), portions_of(number_of, rows * top, most, slope, False)
    places = jnp.arange(number_of)

    def named(lengths, offset_by):
        used = int((lengths > 0).sum())
        fixed = max(1, used // 4)
        shifted = fixed + (places - fixed + offset_by * (used - fixed)) % max(1, number_of - fixed)
        return jnp.zeros((number_of,), jnp.int32).at[order[jnp.where(places < fixed, places, shifted)]].set(jnp.asarray(lengths, jnp.int32))

    lengths = jnp.where(number % 4 == 0, named(packed, number // 4), named(usual, number - number // 4 - 1))
    mixed = jax.random.permutation(jax.random.fold_in(own, 3), number_of)
    donor, receiver = mixed[0:number_of // 2 * 2:2], mixed[1:number_of // 2 * 2:2]
    margin = jnp.minimum(lengths[donor] - 1, most - lengths[receiver]) // 2
    margin = jnp.where((donor == order[0]) | (receiver == order[0]) | (lengths[receiver] == 0), 0, jnp.maximum(margin, 0))
    shifted = jax.random.randint(jax.random.fold_in(own, 4), (number_of // 2,), 0, 1 << 20) % (margin + 1)
    lengths = lengths.at[donor].add(-shifted).at[receiver].add(shifted)
    labels = jnp.searchsorted(jnp.cumsum(lengths), jnp.arange(rows * top), side="right").astype(jnp.int32)
    table = labels.reshape(top, rows).T
    table = table[jax.random.permutation(jax.random.fold_in(own, 1), rows)]
    offset_by = jax.random.randint(jax.random.fold_in(own, 2), (rows, 1), 0, top)
    return jnp.take_along_axis(table, (jnp.arange(top)[None, :] + offset_by) % top, axis=1)


def portions_of(number_of, total, reach, skew, full):
    weights = [(1 << 20) // math.isqrt(standing ** skew) + 1 for standing in range(1, number_of + 1)]
    largest = reach if full else min(reach, max(-(-total // number_of), total * weights[0] // sum(weights)))
    least = 1 if total - largest >= number_of - 1 else 0
    given, rest = [largest] + [least] * (number_of - 1), total - largest - least * (number_of - 1)
    while rest > 0:
        free = [i for i in range(1, number_of) if given[i] < largest] or [i for i in range(1, number_of) if given[i] < reach]
        pool, remaining = sum([weights[i] for i in free]), rest
        for i in free:
            extra = min(reach - given[i], max(1, remaining * weights[i] // pool), rest)
            given[i] = given[i] + extra
            rest = rest - extra
    return np.array(given)


def noise(stream_key, dims, scale, reach, split=(), kind=jnp.bfloat16):
    values = scale * jax.random.normal(stream_key, dims, jnp.float32)
    if split:
        values = values * block_levels(stream_key, dims, split, -0.22, 0.18)
    return jnp.clip(values, -reach, reach).astype(kind)


def setup_inputs(seed: int = 0) -> dict:
    splits = jax.random.split(jax.random.key(seed), 12)
    tokens = noise(splits[0], (TOKENS, D), 1.0, 6.0, ((0, 24),))
    norm_gain = jnp.clip(1.0 + 0.18 * jax.random.normal(splits[1], (D,), jnp.float32), 0.1, 1.9)
    expert_ids_keys = jax.random.split(jax.random.fold_in(splits[2], 1), TOKENS // TOK_G)
    expert_ids_turns = jax.random.permutation(jax.random.fold_in(splits[2], 3), TOKENS // TOK_G)
    expert_ids = jax.vmap(lambda own, number: shared_out(jax.random.fold_in(splits[2], 2), own, number, TOK_G, EXPERTS, 2, CAP, 2))(expert_ids_keys, expert_ids_turns).reshape((TOKENS, 2))
    routing_weight = jnp.clip(0.1 + 0.9 * jax.random.uniform(splits[3], (TOKENS, 2), jnp.float32) ** block_levels(splits[3], (TOKENS, 2), ((0, 24),), -0.2, 0.2), 0.1, 1.0)
    expert_gate = noise(splits[4], (EXPERTS, D, FF), D ** -0.5, 0.125, ((0, 24), (2, 32)))
    expert_up = noise(splits[5], (EXPERTS, D, FF), D ** -0.5, 0.125, ((0, 24), (2, 32)))
    expert_down = noise(splits[6], (EXPERTS, FF, D), FF ** -0.5, 0.078125, ((0, 24), (1, 32)))
    dense_gate_w = noise(splits[7], (D, DS), D ** -0.5, 0.125, ((1, 32),))
    dense_up_w = noise(splits[8], (D, DS), D ** -0.5, 0.125, ((1, 32),))
    dense_down_w = noise(splits[9], (DS, D), DS ** -0.5, 0.1875, ((0, 32),))
    dense_gate = jnp.clip(jax.random.uniform(splits[10], (D,), jnp.float32, -3.0, 3.0) * block_levels(splits[10], (D,), ((0, 32),), -0.4, 0.0), -3.0, 3.0)
    return {"tokens": tokens, "norm_gain": norm_gain, "expert_ids": expert_ids, "routing_weight": routing_weight, "expert_gate": expert_gate, "expert_up": expert_up, "expert_down": expert_down, "dense_gate_w": dense_gate_w, "dense_up_w": dense_up_w, "dense_down_w": dense_down_w, "dense_gate": dense_gate}


EPSILON = 1e-06

def normalize(tokens, norm_gain):
    values = tokens.astype(jnp.float32)
    factor = lax.rsqrt(lax.optimization_barrier(jnp.mean(values * values, axis=-1, keepdims=True)) + EPSILON)
    return (values * factor * norm_gain[None, :]).astype(jnp.bfloat16)

def positions(block_ids):
    flat_ids = block_ids.reshape(-1)
    one_hot = (flat_ids[:, None] == jnp.arange(EXPERTS, dtype=jnp.int32)[None, :]).astype(jnp.int32)
    earlier = jnp.cumsum(one_hot, axis=0) - one_hot
    return flat_ids * CAP + lax.optimization_barrier(jnp.sum(earlier * one_hot, axis=1))

def fill_table(place_row):
    token_no = jnp.arange(2 * TOK_G, dtype=jnp.int32) // 2 + 1
    return jnp.zeros((EXPERTS * CAP,), jnp.int32).at[place_row].set(token_no)

def pick_rows(table, index_row):
    return table[index_row]

def block_sum(hidden, down_w, part_size):
    row_count = hidden.shape[0]
    pieces = hidden.reshape(row_count, N_TP, part_size).astype(jnp.float32)
    weights = down_w.reshape(N_TP, part_size, down_w.shape[1]).astype(jnp.float32)
    partial_value = jnp.einsum('rpf,pfd->rpd', pieces, weights).astype(jnp.bfloat16)
    partial_value = lax.optimization_barrier(partial_value)
    return lax.optimization_barrier(jnp.sum(partial_value.astype(jnp.float32), axis=1))

def reference(tokens, norm_gain, expert_ids, routing_weight, expert_gate, expert_up, expert_down, dense_gate_w, dense_up_w, dense_down_w, dense_gate):
    normed = normalize(tokens, norm_gain)
    normed_blocks = normed.reshape(N_EP, TOK_G, D)
    places = jax.vmap(positions)(expert_ids.reshape(N_EP, TOK_G, 2))
    sources = jax.vmap(fill_table)(places)
    padded = jnp.concatenate([jnp.zeros((N_EP, 1, D), jnp.bfloat16), normed_blocks], axis=1)
    gathered = jax.vmap(pick_rows)(padded, sources)
    expert_rows = gathered.reshape(N_EP, EXPERTS, CAP, D).transpose(1, 0, 2, 3).reshape(EXPERTS, N_EP * CAP, D)

    def one_expert(operands):
        rows_in, gate_w, up_w, down_w = operands
        gate_act = jnp.dot(rows_in, gate_w, preferred_element_type=jnp.float32)
        up_act = jnp.dot(rows_in, up_w, preferred_element_type=jnp.float32)
        hidden = (jax.nn.silu(gate_act) * up_act).astype(jnp.bfloat16)
        return block_sum(hidden, down_w, FF_PART)
    expert_out = lax.map(one_expert, (expert_rows, expert_gate, expert_up, expert_down)).astype(jnp.bfloat16)
    by_source = expert_out.reshape(EXPERTS, N_EP, CAP, D).transpose(1, 0, 2, 3).reshape(N_EP, EXPERTS * CAP, D)
    picked = jax.vmap(pick_rows)(by_source, places).reshape(TOKENS, 2, D).astype(jnp.float32)
    routed = lax.optimization_barrier(jnp.sum(routing_weight[:, :, None] * picked, axis=1))

    def dense_block(block_rows):
        gate_act = jnp.dot(block_rows, dense_gate_w, preferred_element_type=jnp.float32)
        up_act = jnp.dot(block_rows, dense_up_w, preferred_element_type=jnp.float32)
        hidden = (jax.nn.silu(gate_act) * up_act).astype(jnp.bfloat16)
        return block_sum(hidden, dense_down_w, DS_PART)
    dense_out = lax.map(dense_block, normed_blocks).reshape(TOKENS, D)
    layer_out = routed + jax.nn.sigmoid(dense_gate)[None, :] * dense_out
    return layer_out.astype(jnp.bfloat16)
```

```python
import jax
import jax.numpy as jnp
from jax import lax
from jax.sharding import Mesh
from jax.sharding import PartitionSpec as P

TP = ("tp_0", "tp_1")

EPSILON = 1e-06


def positions(block_ids, experts, capacity):
    flat_ids = block_ids.reshape(-1)
    one_hot = (flat_ids[:, None] == jnp.arange(experts, dtype=jnp.int32)[None, :]).astype(jnp.int32)
    earlier = jnp.cumsum(one_hot, axis=0) - one_hot
    return flat_ids * capacity + jnp.sum(earlier * one_hot, axis=1)


def exchange(blocks, axis):
    return lax.all_to_all(blocks, axis, split_axis=0, concat_axis=0, tiled=True)


def copies_from_all(value, axis):
    count = lax.axis_size(axis)
    sent = jnp.broadcast_to(value[None], (count, *value.shape))
    return exchange(sent, axis).reshape(count * value.shape[0], *value.shape[1:])


def sum_at_owner(value, axis):
    count = lax.axis_size(axis)
    blocks = value.reshape(count, value.shape[0] // count, *value.shape[1:])
    return exchange(blocks, axis).astype(jnp.float32).sum(axis=0)


def columns_by_owner(weight, far, near):
    rows, width = weight.shape
    part = width // (far * near)
    return weight.reshape(rows, far, near, part).transpose(0, 2, 1, 3).reshape(rows, width)


def contract_first(left, right):
    return lax.dot_general(left, right, (((0,), (0,)), ((), ())), preferred_element_type=jnp.float32)


def local(
    tokens,
    norm_gain,
    expert_ids,
    routing_weight,
    expert_gate,
    expert_up,
    expert_down,
    dense_gate_w,
    dense_up_w,
    dense_down_w,
    dense_gate,
):
    experts = lax.axis_size("ep")
    far, near = lax.axis_size("tp_0"), lax.axis_size("tp_1")
    group_tokens, model_width = tokens.shape
    capacity = 3 * group_tokens // experts
    slots_all = experts * capacity
    part = model_width // (far * near)
    values = tokens.astype(jnp.float32)
    factor = lax.rsqrt(jnp.mean(values * values, axis=-1, keepdims=True) + EPSILON)
    normed = (values * factor * norm_gain[None, :]).astype(jnp.bfloat16)
    places = positions(expert_ids, experts, capacity)

    token_no = jnp.arange(2 * group_tokens, dtype=jnp.int32) // 2 + 1
    sources = jnp.zeros((slots_all,), jnp.int32).at[places].set(token_no)
    padded = jnp.concatenate([jnp.zeros((1, model_width), jnp.bfloat16), normed], axis=0)
    first = (lax.axis_index("tp_1") * far + lax.axis_index("tp_0")) * part
    column_part = lax.dynamic_slice_in_dim(padded, first, part, 1)
    outgoing = column_part[sources].reshape(experts, capacity * part // 128, 128)
    landed = exchange(outgoing, "ep")
    landed = landed.reshape(slots_all, part).T
    rows_t = copies_from_all(copies_from_all(landed, "tp_0"), "tp_1")

    gate_act = contract_first(expert_gate[0], rows_t)
    up_act = contract_first(expert_up[0], rows_t)
    hidden = (jax.nn.silu(gate_act) * up_act).astype(jnp.bfloat16)
    dense_gate_act = lax.dot_general(
        dense_gate_w, normed, (((0,), (1,)), ((), ())), preferred_element_type=jnp.float32
    )
    dense_up_act = lax.dot_general(
        dense_up_w, normed, (((0,), (1,)), ((), ())), preferred_element_type=jnp.float32
    )
    dense_hidden = (jax.nn.silu(dense_gate_act) * dense_up_act).astype(jnp.bfloat16)

    both_hidden = jnp.concatenate(
        [
            jnp.pad(hidden, ((0, 0), (0, group_tokens))),
            jnp.pad(dense_hidden, ((0, 0), (slots_all, 0))),
        ],
        axis=0,
    )
    both_down = columns_by_owner(jnp.concatenate([expert_down[0], dense_down_w], axis=0), far, near)
    partial = contract_first(both_down, both_hidden).astype(jnp.bfloat16)
    over_near = sum_at_owner(partial, "tp_1").astype(jnp.bfloat16)
    total = sum_at_owner(over_near, "tp_0")
    dense_out = total[:, slots_all:]
    expert_out = total[:, :slots_all].astype(jnp.bfloat16).reshape(part, experts, capacity)
    going_back = expert_out.transpose(1, 2, 0).reshape(experts, capacity * part // 128, 128)
    returned = exchange(going_back, "ep").reshape(slots_all, part)

    picked = jnp.take(returned, places, axis=0).astype(jnp.float32)
    picked = picked.reshape(group_tokens, 2, part)
    routed = jnp.sum(picked * routing_weight[:, :, None], axis=1)
    gate_factor = jax.nn.sigmoid(dense_gate)[None, :]
    return (routed + gate_factor * dense_out.T).astype(jnp.bfloat16)


def solution(mesh):
    finer = Mesh(mesh.devices.reshape(mesh.shape["ep"], 8, 4), ("ep", "tp_0", "tp_1"))
    in_specs = (
        P("ep", None),
        P(),
        P("ep", None),
        P("ep", None),
        P("ep", None, TP),
        P("ep", None, TP),
        P("ep", TP, None),
        P(None, TP),
        P(None, TP),
        P(TP, None),
        P(TP),
    )
    out_specs = P("ep", TP)
    return jax.shard_map(local, mesh=finer, in_specs=in_specs, out_specs=out_specs, check_vma=False)
```

```python
import jax
import jax.numpy as jnp
from jax import lax
from jax.sharding import Mesh
from jax.sharding import PartitionSpec as P

TP = ("yh", "yl", "xh", "xl")
FAR, NEAR = 8, 4

EPSILON = 1e-06


def exchange(blocks, axes):
    return lax.all_to_all(blocks, axes, split_axis=0, concat_axis=0, tiled=True)


def to_neighbour(value, dy, dx):
    pairs = [
        (y * NEAR + x, (y + dy) % FAR * NEAR + (x + dx) % NEAR)
        for y in range(FAR)
        for x in range(NEAR)
    ]
    return lax.ppermute(value, TP, pairs)


def dot(left, right, left_dim, right_dim):
    return lax.dot_general(
        left, right, (((left_dim,), (right_dim,)), ((), ())), preferred_element_type=jnp.float32
    )


def slots_of(ids, experts, capacity):
    tokens = ids.shape[1]
    named = ids[:, None, :] == jnp.arange(experts, dtype=jnp.int32)[None, :, None]
    count = (named[0] | named[1]).astype(jnp.bfloat16)
    before = lax.broadcasted_iota(jnp.int32, (tokens, tokens), 0) < lax.broadcasted_iota(
        jnp.int32, (tokens, tokens), 1
    )
    earlier = dot(count, before.astype(jnp.bfloat16), 1, 0).astype(jnp.int32)
    return ids * capacity + jnp.sum(jnp.where(named, earlier[None], 0), axis=1)


def glu(rows, gates, ups):
    gate_act = sum(dot(r, g, 1, 0) for r, g in zip(rows, gates))
    up_act = sum(dot(r, u, 1, 0) for r, u in zip(rows, ups))
    return (jax.nn.silu(gate_act) * up_act).astype(jnp.bfloat16)


def local(
    tokens,
    norm_gain,
    expert_ids,
    routing_weight,
    expert_gate,
    expert_up,
    expert_down,
    dense_gate_w,
    dense_up_w,
    dense_down_w,
    dense_gate,
):
    experts = lax.axis_size("ep")
    group_tokens, model_width = tokens.shape
    capacity = 3 * group_tokens // experts
    slots_all = experts * capacity
    half = slots_all // 2
    part = model_width // (FAR * NEAR)
    wide = model_width // 4
    mine = lax.axis_index("yl") * 2 + lax.axis_index("xl")

    def of_class(weight, k, dim):
        return lax.dynamic_slice_in_dim(weight, (mine ^ k) * wide, wide, dim)

    values = tokens.astype(jnp.float32)
    factor = lax.rsqrt(jnp.mean(values * values, axis=-1, keepdims=True) + EPSILON)
    normed = (values * factor * norm_gain[None, :]).astype(jnp.bfloat16)
    places = slots_of(expert_ids.T, experts, capacity)
    slot_no = lax.broadcasted_iota(jnp.int32, (slots_all, group_tokens), 0)
    chosen = [(places[c][None, :] == slot_no).astype(jnp.bfloat16) for c in range(2)]
    outgoing = dot(chosen[0] + chosen[1], of_class(normed, 0, 1), 1, 0).astype(jnp.bfloat16)
    landed = exchange(outgoing.reshape(experts, capacity, wide), "ep").reshape(slots_all, wide)

    dense_hidden = glu([normed], [dense_gate_w], [dense_up_w])

    def by_class(weight):
        rows = weight.shape[0]
        split = weight.reshape(rows, FAR // 2, 2, NEAR // 2, 2, part)
        return split.transpose(0, 2, 4, 1, 3, 5).reshape(rows, model_width)

    dense_down = by_class(dense_down_w)
    dense_part = [
        dot(of_class(dense_down, k, 1), dense_hidden, 0, 1).astype(jnp.bfloat16) for k in range(4)
    ]
    dense_sum = (
        dense_part[0].astype(jnp.float32)
        + to_neighbour(dense_part[1], 0, 1).astype(jnp.float32)
        + to_neighbour(dense_part[2], 1, 0).astype(jnp.float32)
        + to_neighbour(dense_part[3], 1, 1).astype(jnp.float32)
    ).astype(jnp.bfloat16)

    gates = [of_class(expert_gate[0], k, 0) for k in range(4)]
    ups = [of_class(expert_up[0], k, 0) for k in range(4)]
    down = by_class(expert_down[0])
    downs = [of_class(down, k, 1) for k in range(4)]
    sums = []
    for number, way in enumerate((1, -1)):
        rows = landed[number * half : (number + 1) * half]
        all_rows = [
            rows,
            to_neighbour(rows, 0, way),
            to_neighbour(rows, way, 0),
            to_neighbour(rows, way, way),
        ]
        hidden = glu(all_rows, gates, ups)
        partial = [dot(d, hidden, 0, 1).astype(jnp.bfloat16) for d in downs]
        sums.append(
            (
                partial[0].astype(jnp.float32)
                + to_neighbour(partial[1], 0, way).astype(jnp.float32)
                + to_neighbour(partial[2], way, 0).astype(jnp.float32)
                + to_neighbour(partial[3], way, way).astype(jnp.float32)
            ).astype(jnp.bfloat16)
        )
    over_blocks = jnp.concatenate([*sums, dense_sum], axis=1)
    pieces = exchange(over_blocks.reshape(8, part, slots_all + group_tokens), ("yh", "xh"))
    total = pieces.astype(jnp.float32).sum(axis=0)
    dense_out = total[:, slots_all:]
    expert_out = total[:, :slots_all].astype(jnp.bfloat16)
    going_back = expert_out.T.reshape(experts, capacity * part // 128, 128)
    returned = exchange(going_back, "ep").reshape(slots_all, part)

    routed = sum(
        routing_weight[:, c][None, :] * dot(returned, chosen[c], 0, 0) for c in range(2)
    )
    gate_factor = jax.nn.sigmoid(dense_gate)[:, None]
    return (routed + gate_factor * dense_out).astype(jnp.bfloat16).T


def solution(mesh):
    sizes = (mesh.shape["ep"], FAR // 2, 2, NEAR // 2, 2)
    finer = Mesh(mesh.devices.reshape(sizes), ("ep", *TP))
    in_specs = (
        P("ep", None),
        P(),
        P("ep", None),
        P("ep", None),
        P("ep", None, TP),
        P("ep", None, TP),
        P("ep", TP, None),
        P(None, TP),
        P(None, TP),
        P(TP, None),
        P(TP),
    )
    out_specs = P("ep", TP)
    return jax.shard_map(local, mesh=finer, in_specs=in_specs, out_specs=out_specs, check_vma=False)
```

```python
import jax
import jax.numpy as jnp
from jax import lax
from jax.sharding import Mesh
from jax.sharding import PartitionSpec as P

TP = ("yh", "yl", "xh", "xl")
FAR, NEAR = 8, 4

EPSILON = 1e-06


def exchange(blocks, axes):
    return lax.all_to_all(blocks, axes, split_axis=0, concat_axis=0, tiled=True)


def send(value, target):
    pairs = []
    for y in range(FAR):
        for x in range(NEAR):
            there_y, there_x = target(y, x)
            pairs.append((y * NEAR + x, there_y % FAR * NEAR + there_x % NEAR))
    return lax.ppermute(value, TP, pairs)


def pair(y, x):
    return y, x ^ 1


def across(x):
    return x + (1 if x % 2 else -1)


def up_one(y, x):
    return y + 1, across(x)


def down_one(y, x):
    return y - 1, across(x)


def up_two(y, x):
    return y + 2, x


def down_two(y, x):
    return y - 2, x


def dot(left, right, left_dim, right_dim):
    return lax.dot_general(
        left, right, (((left_dim,), (right_dim,)), ((), ())), preferred_element_type=jnp.float32
    )


def slots_of(ids, experts):
    tokens = ids.shape[1]
    named = ids[:, None, :] == jnp.arange(experts, dtype=jnp.int32)[None, :, None]
    count = (named[0] | named[1]).astype(jnp.bfloat16)
    before = lax.broadcasted_iota(jnp.int32, (tokens, tokens), 0) < lax.broadcasted_iota(
        jnp.int32, (tokens, tokens), 1
    )
    earlier = dot(count, before.astype(jnp.bfloat16), 1, 0).astype(jnp.int32)
    return jnp.sum(jnp.where(named, earlier[None], 0), axis=1)


def silu_times(gate_act, up_act):
    return (jax.nn.silu(gate_act) * up_act).astype(jnp.bfloat16)


def total_of(terms):
    return sum(term.astype(jnp.float32) for term in terms).astype(jnp.bfloat16)


def by_class(weight):
    run = weight.shape[1] // FAR
    order = [(m + 4 * high) * run for m in range(4) for high in range(2)]
    return jnp.concatenate([weight[:, first : first + run] for first in order], axis=1)


def local(
    tokens,
    norm_gain,
    expert_ids,
    routing_weight,
    expert_gate,
    expert_up,
    expert_down,
    dense_gate_w,
    dense_up_w,
    dense_down_w,
    dense_gate,
):
    experts = lax.axis_size("ep")
    group_tokens, model_width = tokens.shape
    capacity = 3 * group_tokens // experts
    few = capacity // 2
    rows_mine = experts * few
    part = model_width // (FAR * NEAR)
    wide = model_width // 4
    hidden_part = expert_gate.shape[2]
    x_at = lax.axis_index("xh") * 2 + lax.axis_index("xl")
    mine = lax.axis_index("yl")
    color = (x_at + mine) % 2
    far_at = lax.axis_index("yh") * 2 + lax.axis_index("xh")

    own_w = [expert_gate[0].T, expert_up[0].T, by_class(expert_down[0])]
    swapped = send(jnp.concatenate(own_w, axis=0), pair)
    other_w = [swapped[i * hidden_part : (i + 1) * hidden_part] for i in range(3)]

    def of_class(weight, step, dim):
        return lax.dynamic_slice_in_dim(weight, (mine + step) % 4 * wide, wide, dim)

    values = tokens.astype(jnp.float32)
    factor = lax.rsqrt(jnp.mean(values * values, axis=-1, keepdims=True) + EPSILON)
    normed = (values * factor * norm_gain[None, :]).astype(jnp.bfloat16)
    ids = expert_ids.T
    shifted = slots_of(ids, experts) - color * few
    places = jnp.where((shifted >= 0) & (shifted < few), ids * few + shifted, -1)
    slot_no = lax.broadcasted_iota(jnp.int32, (rows_mine, group_tokens), 0)
    chosen = [(places[c][None, :] == slot_no).astype(jnp.bfloat16) for c in range(2)]
    outgoing = dot(chosen[0] + chosen[1], of_class(normed, 0, 1), 1, 0).astype(jnp.bfloat16)
    landed = exchange(outgoing.reshape(experts, few, wide), "ep").reshape(rows_mine, wide)

    dense_hidden = silu_times(dot(normed, dense_gate_w, 1, 0), dot(normed, dense_up_w, 1, 0))
    dense_down = by_class(dense_down_w)
    dense_part = [
        dot(of_class(dense_down, step, 1), dense_hidden, 0, 1).astype(jnp.bfloat16)
        for step in range(4)
    ]
    dense_sum = total_of(
        [
            dense_part[0],
            send(dense_part[1], up_one),
            send(dense_part[2], up_two),
            send(dense_part[3], down_one),
        ]
    )
    dense_pieces = exchange(dense_sum.reshape(8, part, group_tokens), ("yh", "xh", "xl"))
    dense_out = dense_pieces.astype(jnp.float32).sum(axis=0)

    block = rows_mine // 2
    arrived = [
        landed,
        send(landed, up_one),
        jnp.concatenate([send(landed[:block], up_two), send(landed[block:], down_two)], axis=0),
        send(landed, down_one),
    ]

    def hidden_of(weights):
        gate_act = sum(dot(r, of_class(weights[0], -k, 1), 1, 1) for k, r in enumerate(arrived))
        up_act = sum(dot(r, of_class(weights[1], -k, 1), 1, 1) for k, r in enumerate(arrived))
        return silu_times(gate_act, up_act)

    own_hidden, other_hidden = hidden_of(own_w), hidden_of(other_w)
    partial = [
        (
            dot(own_hidden, of_class(own_w[2], step, 1), 1, 0)
            + dot(other_hidden, of_class(other_w[2], step, 1), 1, 0)
        ).astype(jnp.bfloat16)
        for step in range(4)
    ]
    back_two = [send(partial[2][:block], up_two), send(partial[2][block:], down_two)]
    near_sum = total_of(
        [
            partial[0],
            jnp.concatenate(back_two, axis=0),
            send(partial[1], up_one),
            send(partial[3], down_one),
        ]
    )

    def far_piece(step):
        return lax.dynamic_slice_in_dim(near_sum, (far_at ^ step) * 2 * part, 2 * part, 1)

    expert_out = total_of(
        [
            far_piece(0),
            send(far_piece(1), lambda y, x: (y, x + 2)),
            send(far_piece(2), lambda y, x: (y + 4, x)),
            send(far_piece(3), lambda y, x: (y + 4, x + 2)),
        ]
    )
    returned = exchange(expert_out.reshape(experts, few, 2 * part), "ep")
    returned = returned.reshape(rows_mine, 2 * part)
    weight = routing_weight.T
    routed = sum(weight[c][None, :] * dot(returned, chosen[c], 0, 0) for c in range(2))
    keep = lax.dynamic_slice_in_dim(routed, x_at % 2 * part, part, 0)
    give = lax.dynamic_slice_in_dim(routed, (1 - x_at % 2) * part, part, 0)
    routed = keep + send(give.astype(jnp.bfloat16), pair).astype(jnp.float32)
    gate_factor = jax.nn.sigmoid(dense_gate)[:, None]
    return (routed + gate_factor * dense_out).astype(jnp.bfloat16).T


def solution(mesh):
    sizes = (mesh.shape["ep"], FAR // 4, 4, NEAR // 2, 2)
    finer = Mesh(mesh.devices.reshape(sizes), ("ep", *TP))
    in_specs = (
        P("ep", None),
        P(),
        P("ep", None),
        P("ep", None),
        P("ep", None, TP),
        P("ep", None, TP),
        P("ep", TP, None),
        P(None, TP),
        P(None, TP),
        P(TP, None),
        P(TP),
    )
    out_specs = P("ep", TP)
    return jax.shard_map(local, mesh=finer, in_specs=in_specs, out_specs=out_specs, check_vma=False)
```

```python
import jax
import jax.numpy as jnp
from jax import lax
from jax.sharding import Mesh
from jax.sharding import PartitionSpec as P

TP = ("ya", "yb", "yc", "xh", "xl")
FAR, NEAR = 8, 4

EPSILON = 1e-06


def exchange(blocks, axes):
    return lax.all_to_all(blocks, axes, split_axis=0, concat_axis=0, tiled=True)


def send(value, target):
    pairs = []
    for y in range(FAR):
        for x in range(NEAR):
            there_y, there_x = target(y, x)
            pairs.append((y * NEAR + x, there_y % FAR * NEAR + there_x % NEAR))
    return lax.ppermute(value, TP, pairs)


def along_y(steps):
    return lambda y, x: (y + steps, x)


def dot(left, right, left_dim, right_dim):
    return lax.dot_general(
        left, right, (((left_dim,), (right_dim,)), ((), ())), preferred_element_type=jnp.float32
    )


def slots_of(ids, experts):
    tokens = ids.shape[1]
    named = ids[:, None, :] == jnp.arange(experts, dtype=jnp.int32)[None, :, None]
    count = (named[0] | named[1]).astype(jnp.bfloat16)
    before = lax.broadcasted_iota(jnp.int32, (tokens, tokens), 0) < lax.broadcasted_iota(
        jnp.int32, (tokens, tokens), 1
    )
    earlier = dot(count, before.astype(jnp.bfloat16), 1, 0).astype(jnp.int32)
    return jnp.sum(jnp.where(named, earlier[None], 0), axis=1)


def silu_times(gate_act, up_act):
    return (jax.nn.silu(gate_act) * up_act).astype(jnp.bfloat16)


def total_of(terms):
    return sum(term.astype(jnp.float32) for term in terms).astype(jnp.bfloat16)


def columns(weight, starts, size):
    return jnp.concatenate(
        [lax.dynamic_slice_in_dim(weight, start, size, 1) for start in starts], axis=1
    )


def local(
    tokens,
    norm_gain,
    expert_ids,
    routing_weight,
    expert_gate,
    expert_up,
    expert_down,
    dense_gate_w,
    dense_up_w,
    dense_down_w,
    dense_gate,
):
    experts = lax.axis_size("ep")
    group_tokens, model_width = tokens.shape
    capacity = 3 * group_tokens // experts
    few = capacity // 2
    rows_mine = experts * few
    part = model_width // (FAR * NEAR)
    wide = model_width // 4
    row_width = model_width // FAR
    hidden_part = expert_gate.shape[2]
    odd_y, odd_x = lax.axis_index("yc"), lax.axis_index("xl")
    mod_y = lax.axis_index("yb") * 2 + odd_y

    own_w = [expert_gate[0].T, expert_up[0].T, expert_down[0]]
    swapped = send(jnp.concatenate(own_w, axis=0), lambda y, x: (y, x ^ 1))
    other_w = [swapped[i * hidden_part : (i + 1) * hidden_part] for i in range(3)]

    values = tokens.astype(jnp.float32)
    factor = lax.rsqrt(jnp.mean(values * values, axis=-1, keepdims=True) + EPSILON)
    normed = (values * factor * norm_gain[None, :]).astype(jnp.bfloat16)
    ids = expert_ids.T
    shifted = slots_of(ids, experts) - odd_x * few
    places = jnp.where((shifted >= 0) & (shifted < few), ids * few + shifted, -1)
    slot_no = lax.broadcasted_iota(jnp.int32, (rows_mine, group_tokens), 0)
    chosen = [(places[c][None, :] == slot_no).astype(jnp.bfloat16) for c in range(2)]

    def side(weight, other):
        return lax.dynamic_slice_in_dim(weight, (odd_y ^ other) * 2 * wide, 2 * wide, 1)

    outgoing = dot(chosen[0] + chosen[1], side(normed, 0), 1, 0).astype(jnp.bfloat16)
    landed = exchange(outgoing.reshape(experts, few, 2 * wide), "ep")
    landed = landed.reshape(rows_mine, 2 * wide)

    dense_hidden = silu_times(dot(normed, dense_gate_w, 1, 0), dot(normed, dense_up_w, 1, 0))

    def dense_part(step):
        first = (mod_y + step) % 4 * row_width
        down = columns(dense_down_w, [first, first + 4 * row_width], row_width)
        return dot(down, dense_hidden, 0, 1).astype(jnp.bfloat16)

    dense_terms = [
        send(dense_part(1), along_y(1)),
        send(dense_part(2), along_y(2)),
        send(dense_part(3), along_y(-1)),
    ]
    dense_sum = total_of([dense_part(0), *dense_terms])
    dense_pieces = exchange(dense_sum.reshape(8, part, group_tokens), ("ya", "xh", "xl"))
    dense_out = dense_pieces.astype(jnp.float32).sum(axis=0)

    block = rows_mine // 2
    arrived = [send(landed[:block], along_y(1)), send(landed[block:], along_y(-1))]

    def hidden_of(weights):
        halves = []
        for i in range(2):
            rows = [landed[i * block : (i + 1) * block], arrived[i]]
            gate_act = sum(dot(r, side(weights[0], k), 1, 1) for k, r in enumerate(rows))
            up_act = sum(dot(r, side(weights[1], k), 1, 1) for k, r in enumerate(rows))
            halves.append(silu_times(gate_act, up_act))
        return jnp.concatenate(halves, axis=0)

    own_hidden = hidden_of(own_w)
    other_hidden = hidden_of(other_w)
    partial = dot(own_w[2], own_hidden, 0, 1) + dot(other_w[2], other_hidden, 0, 1)
    partial = partial.astype(jnp.bfloat16).reshape(4, 2, 2, 2 * part, rows_mine)
    partial = partial.transpose(1, 2, 0, 3, 4).reshape(4, wide, rows_mine)
    near_terms = exchange(partial, ("yc", "xh"))
    near_sum = total_of([near_terms[k] for k in range(4)])
    returned = exchange(near_sum.T.reshape(experts, few, wide), "ep")
    returned = returned.reshape(rows_mine, wide)
    weight = routing_weight.T
    routed = sum(weight[c][None, :] * dot(returned, chosen[c], 0, 0) for c in range(2))
    pieces = exchange(
        routed.astype(jnp.bfloat16).reshape(8, part, group_tokens), ("ya", "yb", "xl")
    )
    routed = pieces.astype(jnp.float32).sum(axis=0)
    gate_factor = jax.nn.sigmoid(dense_gate)[:, None]
    return (routed + gate_factor * dense_out).astype(jnp.bfloat16).T


def solution(mesh):
    finer = Mesh(mesh.devices.reshape(mesh.shape["ep"], 2, 2, 2, 2, 2), ("ep", *TP))
    in_specs = (
        P("ep", None),
        P(),
        P("ep", None),
        P("ep", None),
        P("ep", None, TP),
        P("ep", None, TP),
        P("ep", TP, None),
        P(None, TP),
        P(None, TP),
        P(TP, None),
        P(TP),
    )
    out_specs = P("ep", TP)
    return jax.shard_map(local, mesh=finer, in_specs=in_specs, out_specs=out_specs, check_vma=False)
```

```python
import jax
import jax.numpy as jnp
from jax import lax
from jax.sharding import Mesh
from jax.sharding import PartitionSpec as P

TP = ("ya", "yb", "yc", "xh", "xl")
FAR, NEAR = 8, 4

EPSILON = 1e-06


def exchange(blocks, axes):
    return lax.all_to_all(blocks, axes, split_axis=0, concat_axis=0, tiled=True)


def send(value, target):
    pairs = []
    for y in range(FAR):
        for x in range(NEAR):
            there_y, there_x = target(y, x)
            pairs.append((y * NEAR + x, there_y % FAR * NEAR + there_x % NEAR))
    return lax.ppermute(value, TP, pairs)


def along_y(steps):
    return lambda y, x: (y + steps, x)


def dot(left, right, left_dim, right_dim):
    return lax.dot_general(
        left, right, (((left_dim,), (right_dim,)), ((), ())), preferred_element_type=jnp.float32
    )


def slots_of(ids, experts):
    tokens = ids.shape[1]
    named = ids[:, None, :] == jnp.arange(experts, dtype=jnp.int32)[None, :, None]
    count = (named[0] | named[1]).astype(jnp.bfloat16)
    before = lax.broadcasted_iota(jnp.int32, (tokens, tokens), 0) < lax.broadcasted_iota(
        jnp.int32, (tokens, tokens), 1
    )
    earlier = dot(count, before.astype(jnp.bfloat16), 1, 0).astype(jnp.int32)
    return jnp.sum(jnp.where(named, earlier[None], 0), axis=1)


def silu_times(gate_act, up_act):
    return (jax.nn.silu(gate_act) * up_act).astype(jnp.bfloat16)


def total_of(terms):
    return sum(term.astype(jnp.float32) for term in terms).astype(jnp.bfloat16)


def columns(weight, starts, size):
    return jnp.concatenate(
        [lax.dynamic_slice_in_dim(weight, start, size, 1) for start in starts], axis=1
    )


def local(
    tokens,
    norm_gain,
    expert_ids,
    routing_weight,
    expert_gate,
    expert_up,
    expert_down,
    dense_gate_w,
    dense_up_w,
    dense_down_w,
    dense_gate,
):
    experts = lax.axis_size("ep")
    group_tokens, model_width = tokens.shape
    capacity = 3 * group_tokens // experts
    few = capacity // 2
    rows_mine = experts * few
    part = model_width // (FAR * NEAR)
    wide = model_width // 4
    row_width = model_width // FAR
    hidden_part = expert_gate.shape[2]
    odd_y, odd_x = lax.axis_index("yc"), lax.axis_index("xl")
    mod_y = lax.axis_index("yb") * 2 + odd_y

    own_w = jnp.concatenate([expert_gate[0].T, expert_up[0].T, expert_down[0]], axis=0)
    other_w = send(own_w, lambda y, x: (y, x ^ 1))

    values = tokens.astype(jnp.float32)
    factor = lax.rsqrt(jnp.mean(values * values, axis=-1, keepdims=True) + EPSILON)
    normed = (values * factor * norm_gain[None, :]).astype(jnp.bfloat16)
    ids = expert_ids.T
    shifted = slots_of(ids, experts) - odd_x * few
    places = jnp.where((shifted >= 0) & (shifted < few), ids * few + shifted, -1)
    slot_no = lax.broadcasted_iota(jnp.int32, (rows_mine, group_tokens), 0)
    chosen = [(places[c][None, :] == slot_no).astype(jnp.bfloat16) for c in range(2)]

    def side(weight, other):
        return lax.dynamic_slice_in_dim(weight, (odd_y ^ other) * 2 * wide, 2 * wide, 1)

    outgoing = dot(chosen[0] + chosen[1], side(normed, 0), 1, 0).astype(jnp.bfloat16)
    landed = exchange(outgoing.reshape(experts, few, 2 * wide), "ep")
    landed = landed.reshape(rows_mine, 2 * wide)

    dense_hidden = silu_times(dot(normed, dense_gate_w, 1, 0), dot(normed, dense_up_w, 1, 0))

    def dense_part(step):
        first = (mod_y + step) % 4 * row_width
        down = columns(dense_down_w, [first, first + 4 * row_width], row_width)
        return dot(down, dense_hidden, 0, 1).astype(jnp.bfloat16)

    dense_terms = [
        send(dense_part(1), along_y(1)),
        send(dense_part(2), along_y(2)),
        send(dense_part(3), along_y(-1)),
    ]
    dense_sum = total_of([dense_part(0), *dense_terms])
    dense_sum = dense_sum.reshape(2, NEAR, part, group_tokens)

    def for_x(step):
        there = (lax.axis_index("xh") * 2 + odd_x + step) % NEAR
        return lax.dynamic_index_in_dim(dense_sum, there, 1, keepdims=False)

    dense_x = total_of(
        [for_x(0)] + [send(for_x(k), lambda y, x, k=k: (y, x + k)) for k in range(1, NEAR)]
    )
    high = lax.axis_index("ya")
    dense_mine = lax.dynamic_index_in_dim(dense_x, high, 0, keepdims=False)
    dense_theirs = lax.dynamic_index_in_dim(dense_x, 1 - high, 0, keepdims=False)
    dense_theirs = send(dense_theirs, along_y(4))
    dense_out = dense_mine.astype(jnp.float32) + dense_theirs.astype(jnp.float32)

    arrived = [send(landed[:, :wide], along_y(1)), send(landed[:, wide:], along_y(-1))]

    def hidden_of(weights):
        gate_up = weights[: 2 * hidden_part]
        act = dot(side(gate_up, 0), landed, 1, 1)
        beside = side(gate_up, 1)
        for i in range(2):
            act = act + dot(beside[:, i * wide : (i + 1) * wide], arrived[i], 1, 1)
        return silu_times(act[:hidden_part], act[hidden_part:])

    own_hidden = hidden_of(own_w)
    other_hidden = hidden_of(other_w)
    partial = dot(own_w[2 * hidden_part :], own_hidden, 0, 0)
    partial = partial + dot(other_w[2 * hidden_part :], other_hidden, 0, 0)
    partial = partial.astype(jnp.bfloat16).reshape(4, 2, 2, 2 * part, rows_mine)
    partial = partial.transpose(1, 2, 0, 3, 4).reshape(4, wide, rows_mine)
    near_terms = exchange(partial, ("yc", "xh"))
    near_sum = total_of([near_terms[k] for k in range(4)])
    returned = exchange(near_sum.T.reshape(experts, few, wide), "ep")
    returned = returned.reshape(rows_mine, wide)
    weight = routing_weight.T
    routed = sum(weight[c][None, :] * dot(returned, chosen[c], 0, 0) for c in range(2))
    pieces = exchange(
        routed.astype(jnp.bfloat16).reshape(8, part, group_tokens), ("ya", "yb", "xl")
    )
    routed = pieces.astype(jnp.float32).sum(axis=0)
    gate_factor = jax.nn.sigmoid(dense_gate)[:, None]
    return (routed + gate_factor * dense_out).astype(jnp.bfloat16).T


def solution(mesh):
    finer = Mesh(mesh.devices.reshape(mesh.shape["ep"], 2, 2, 2, 2, 2), ("ep", *TP))
    in_specs = (
        P("ep", None),
        P(),
        P("ep", None),
        P("ep", None),
        P("ep", None, TP),
        P("ep", None, TP),
        P("ep", TP, None),
        P(None, TP),
        P(None, TP),
        P(TP, None),
        P(TP),
    )
    out_specs = P("ep", TP)
    return jax.shard_map(local, mesh=finer, in_specs=in_specs, out_specs=out_specs, check_vma=False)
```

```python
import jax
import jax.numpy as jnp
from jax import lax
from jax.experimental import pallas as pl
from jax.experimental.pallas import tpu as pltpu
from jax.sharding import Mesh
from jax.sharding import PartitionSpec as P

TP = ("ya", "yb", "yc", "xh", "xl")
FAR, NEAR = 8, 4

EPSILON = 1e-06


def exchange(blocks, axes):
    return lax.all_to_all(blocks, axes, split_axis=0, concat_axis=0, tiled=True)


def send(value, target):
    pairs = []
    for y in range(FAR):
        for x in range(NEAR):
            there_y, there_x = target(y, x)
            pairs.append((y * NEAR + x, there_y % FAR * NEAR + there_x % NEAR))
    return lax.ppermute(value, TP, pairs)


def along_y(steps):
    return lambda y, x: (y + steps, x)


def dot(left, right, left_dim, right_dim):
    return lax.dot_general(
        left, right, (((left_dim,), (right_dim,)), ((), ())), preferred_element_type=jnp.float32
    )


def slots_of(ids, experts):
    tokens = ids.shape[1]
    named = ids[:, None, :] == jnp.arange(experts, dtype=jnp.int32)[None, :, None]
    count = (named[0] | named[1]).astype(jnp.bfloat16)
    before = lax.broadcasted_iota(jnp.int32, (tokens, tokens), 0) < lax.broadcasted_iota(
        jnp.int32, (tokens, tokens), 1
    )
    earlier = dot(count, before.astype(jnp.bfloat16), 1, 0).astype(jnp.int32)
    return jnp.sum(jnp.where(named, earlier[None], 0), axis=1)


def silu_times(gate_act, up_act):
    return (jax.nn.silu(gate_act) * up_act).astype(jnp.bfloat16)


def total_of(terms):
    return sum(term.astype(jnp.float32) for term in terms).astype(jnp.bfloat16)


def columns(weight, starts, size):
    return jnp.concatenate(
        [lax.dynamic_slice_in_dim(weight, start, size, 1) for start in starts], axis=1
    )


def ffn_kernel(
    place, near_rows, below, above, gate, up, down, first, second, out_0, out_1, out_2, out_3
):
    odd_y, half_x = place[0], place[1]
    width = near_rows.shape[1]
    half = width // 2
    near = pl.multiple_of(odd_y * width, 128)
    beside = pl.multiple_of((1 - odd_y) * width, 128)

    def product(ref, start, count):
        rows = pl.ds(start, count)
        return (
            dot(near_rows[...], ref[rows, pl.ds(near, width)], 1, 1)
            + dot(below[...], ref[rows, pl.ds(beside, half)], 1, 1)
            + dot(above[...], ref[rows, pl.ds(pl.multiple_of(beside + half, 128), half)], 1, 1)
        )

    pieces = []
    own = gate.shape[0]
    hidden = silu_times(product(gate, 0, own), product(up, 0, own))
    pieces.append((hidden, down, 0, own))
    for ref in (first, second):
        count = ref.shape[0] // 3
        hidden = silu_times(product(ref, 0, count), product(ref, count, count))
        pieces.append((hidden, ref, 2 * count, count))
    for k, out in enumerate((out_0, out_1, out_2, out_3)):
        y_bit, x_bit = odd_y ^ (k & 1), half_x ^ (k >> 1)
        total = None
        for hidden, ref, start, count in pieces:
            picked = [
                ref[
                    pl.ds(start, count),
                    pl.ds(pl.multiple_of(((2 * q + y_bit) * 2 + x_bit) * 128, 128), 128),
                ]
                for q in range(4)
            ]
            term = dot(hidden, jnp.concatenate(picked, axis=1), 1, 0)
            total = term if total is None else total + term
        out[...] = total.astype(jnp.bfloat16)


def ffn(place, near_rows, below, above, gate, up, down, first, second):
    rows = near_rows.shape[0]
    wide = down.shape[1] // 4
    in_vmem = pl.BlockSpec(memory_space=pltpu.VMEM)
    units = gate.shape[0] + (first.shape[0] + second.shape[0]) // 3
    return pl.pallas_call(
        ffn_kernel,
        out_shape=[jax.ShapeDtypeStruct((rows, wide), jnp.bfloat16)] * 4,
        in_specs=[pl.BlockSpec(memory_space=pltpu.SMEM)] + [in_vmem] * 8,
        out_specs=[in_vmem] * 4,
        cost_estimate=pl.CostEstimate(
            flops=6 * rows * units * down.shape[1],
            bytes_accessed=2 * down.shape[1] * (3 * units + 2 * rows),
            transcendentals=rows * units,
        ),
        compiler_params=pltpu.CompilerParams(vmem_limit_bytes=24 * 1024 * 1024),
        name="ffn",
    )(place, near_rows, below, above, gate, up, down, first, second)


def local(
    tokens,
    norm_gain,
    expert_ids,
    routing_weight,
    expert_gate,
    expert_up,
    expert_down,
    dense_gate_w,
    dense_up_w,
    dense_down_w,
    dense_gate,
):
    experts = lax.axis_size("ep")
    group_tokens, model_width = tokens.shape
    capacity = 3 * group_tokens // experts
    few = capacity // 2
    rows_mine = experts * few
    part = model_width // (FAR * NEAR)
    wide = model_width // 4
    row_width = model_width // FAR
    hidden_part = expert_gate.shape[2]
    odd_y, odd_x = lax.axis_index("yc"), lax.axis_index("xl")
    mod_y = lax.axis_index("yb") * 2 + odd_y

    gate_t, up_t, down = expert_gate[0].T, expert_up[0].T, expert_down[0]
    split = (hidden_part // 2 + 15) // 16 * 16

    def packed(first, last):
        return jnp.concatenate([w[first:last] for w in (gate_t, up_t, down)], axis=0)

    first_w = send(packed(0, split), lambda y, x: (y, x ^ 1))
    second_w = send(packed(split, hidden_part), lambda y, x: (y, x + (1 if x % 2 else -1)))

    values = tokens.astype(jnp.float32)
    factor = lax.rsqrt(jnp.mean(values * values, axis=-1, keepdims=True) + EPSILON)
    normed = (values * factor * norm_gain[None, :]).astype(jnp.bfloat16)
    ids = expert_ids.T
    shifted = slots_of(ids, experts) - odd_x * few
    places = jnp.where((shifted >= 0) & (shifted < few), ids * few + shifted, -1)
    slot_no = lax.broadcasted_iota(jnp.int32, (rows_mine, group_tokens), 0)
    chosen = [(places[c][None, :] == slot_no).astype(jnp.bfloat16) for c in range(2)]

    def side(weight, other):
        return lax.dynamic_slice_in_dim(weight, (odd_y ^ other) * 2 * wide, 2 * wide, 1)

    outgoing = dot(chosen[0] + chosen[1], side(normed, 0), 1, 0).astype(jnp.bfloat16)
    landed = exchange(outgoing.reshape(experts, few, 2 * wide), "ep")
    landed = landed.reshape(rows_mine, 2 * wide)

    dense_hidden = silu_times(dot(normed, dense_gate_w, 1, 0), dot(normed, dense_up_w, 1, 0))

    def dense_part(step):
        first = (mod_y + step) % 4 * row_width
        down = columns(dense_down_w, [first, first + 4 * row_width], row_width)
        return dot(down, dense_hidden, 0, 1).astype(jnp.bfloat16)

    dense_terms = [
        send(dense_part(1), along_y(1)),
        send(dense_part(2), along_y(2)),
        send(dense_part(3), along_y(-1)),
    ]
    dense_sum = total_of([dense_part(0), *dense_terms])
    dense_sum = dense_sum.reshape(2, NEAR, part, group_tokens)

    def for_x(step):
        there = (lax.axis_index("xh") * 2 + odd_x + step) % NEAR
        return lax.dynamic_index_in_dim(dense_sum, there, 1, keepdims=False)

    dense_x = total_of(
        [for_x(0)] + [send(for_x(k), lambda y, x, k=k: (y, x + k)) for k in range(1, NEAR)]
    )
    high = lax.axis_index("ya")
    dense_mine = lax.dynamic_index_in_dim(dense_x, high, 0, keepdims=False)
    dense_theirs = lax.dynamic_index_in_dim(dense_x, 1 - high, 0, keepdims=False)
    dense_theirs = send(dense_theirs, along_y(4))
    dense_out = dense_mine.astype(jnp.float32) + dense_theirs.astype(jnp.float32)

    arrived = [send(landed[:, :wide], along_y(1)), send(landed[:, wide:], along_y(-1))]

    place = jnp.stack([odd_y, lax.axis_index("xh")])
    out = ffn(place, landed, *arrived, gate_t, up_t, down, first_w, second_w)
    back = [
        send(out[1], lambda y, x: (y + 1, x)),
        send(out[3], lambda y, x: (y + 1, x + 2)),
        send(out[2], lambda y, x: (y, x + 2)),
    ]
    near_sum = total_of([out[0], *back])
    returned = exchange(near_sum.reshape(experts, few, wide), "ep")
    returned = returned.reshape(rows_mine, wide)
    weight = routing_weight.T
    routed = sum(weight[c][None, :] * dot(returned, chosen[c], 0, 0) for c in range(2))
    pieces = exchange(
        routed.astype(jnp.bfloat16).reshape(8, part, group_tokens), ("ya", "yb", "xl")
    )
    routed = pieces.astype(jnp.float32).sum(axis=0)
    gate_factor = jax.nn.sigmoid(dense_gate)[:, None]
    return (routed + gate_factor * dense_out).astype(jnp.bfloat16).T


def solution(mesh):
    finer = Mesh(mesh.devices.reshape(mesh.shape["ep"], 2, 2, 2, 2, 2), ("ep", *TP))
    in_specs = (
        P("ep", None),
        P(),
        P("ep", None),
        P("ep", None),
        P("ep", None, TP),
        P("ep", None, TP),
        P("ep", TP, None),
        P(None, TP),
        P(None, TP),
        P(TP, None),
        P(TP),
    )
    out_specs = P("ep", TP)
    return jax.shard_map(local, mesh=finer, in_specs=in_specs, out_specs=out_specs, check_vma=False)
```

```python
import jax
import jax.numpy as jnp
from jax import lax
from jax.experimental import pallas as pl
from jax.experimental.pallas import tpu as pltpu
from jax.sharding import Mesh
from jax.sharding import PartitionSpec as P

TP = ("ya", "yb", "yc", "xh", "xl")
FAR, NEAR = 8, 4

EPSILON = 1e-06


def exchange(blocks, axes):
    return lax.all_to_all(blocks, axes, split_axis=0, concat_axis=0, tiled=True)


def send(value, target):
    pairs = []
    for y in range(FAR):
        for x in range(NEAR):
            there_y, there_x = target(y, x)
            pairs.append((y * NEAR + x, there_y % FAR * NEAR + there_x % NEAR))
    return lax.ppermute(value, TP, pairs)


def along_y(steps):
    return lambda y, x: (y + steps, x)


def dot(left, right, left_dim, right_dim):
    return lax.dot_general(
        left, right, (((left_dim,), (right_dim,)), ((), ())), preferred_element_type=jnp.float32
    )


def slots_of(ids, experts):
    tokens = ids.shape[1]
    named = ids[:, None, :] == jnp.arange(experts, dtype=jnp.int32)[None, :, None]
    count = (named[0] | named[1]).astype(jnp.bfloat16)
    before = lax.broadcasted_iota(jnp.int32, (tokens, tokens), 0) < lax.broadcasted_iota(
        jnp.int32, (tokens, tokens), 1
    )
    earlier = dot(count, before.astype(jnp.bfloat16), 1, 0).astype(jnp.int32)
    return jnp.sum(jnp.where(named, earlier[None], 0), axis=1)


def silu_times(gate_act, up_act):
    return (jax.nn.silu(gate_act) * up_act).astype(jnp.bfloat16)


def total_of(terms):
    return sum(term.astype(jnp.float32) for term in terms).astype(jnp.bfloat16)


def columns(weight, starts, size):
    return jnp.concatenate(
        [lax.dynamic_slice_in_dim(weight, start, size, 1) for start in starts], axis=1
    )


def ffn_kernel(
    place, near_rows, below, above, gate, up, down, first, second, out
):
    odd_y = place[0]
    width = near_rows.shape[1]
    half = width // 2
    near = pl.multiple_of(odd_y * width, 128)
    beside = pl.multiple_of((1 - odd_y) * width, 128)

    def product(ref, start, count):
        rows = pl.ds(start, count)
        return (
            dot(near_rows[...], ref[rows, pl.ds(near, width)], 1, 1)
            + dot(below[...], ref[rows, pl.ds(beside, half)], 1, 1)
            + dot(above[...], ref[rows, pl.ds(pl.multiple_of(beside + half, 128), half)], 1, 1)
        )

    pieces = []
    own = gate.shape[0]
    hidden = silu_times(product(gate, 0, own), product(up, 0, own))
    pieces.append((hidden, down, 0, own))
    for ref in (first, second):
        count = ref.shape[0] // 3
        hidden = silu_times(product(ref, 0, count), product(ref, count, count))
        pieces.append((hidden, ref, 2 * count, count))
    for q in range(4):
        for y_bit in range(2):
            columns_of = pl.ds((2 * q + y_bit) * 256, 256)
            total = sum(
                dot(hidden, ref[pl.ds(start, count), columns_of], 1, 0)
                for hidden, ref, start, count in pieces
            ).astype(jnp.bfloat16)
            for x_bit in range(2):
                out[2 * y_bit + x_bit, q] = total[:, x_bit * 128 : (x_bit + 1) * 128]


def ffn(place, near_rows, below, above, gate, up, down, first, second):
    rows = near_rows.shape[0]
    in_vmem = pl.BlockSpec(memory_space=pltpu.VMEM)
    units = gate.shape[0] + (first.shape[0] + second.shape[0]) // 3
    return pl.pallas_call(
        ffn_kernel,
        out_shape=jax.ShapeDtypeStruct((4, 4, rows, down.shape[1] // 16), jnp.bfloat16),
        in_specs=[pl.BlockSpec(memory_space=pltpu.SMEM)] + [in_vmem] * 8,
        out_specs=in_vmem,
        cost_estimate=pl.CostEstimate(
            flops=6 * rows * units * down.shape[1],
            bytes_accessed=2 * down.shape[1] * (3 * units + 2 * rows),
            transcendentals=rows * units,
        ),
        compiler_params=pltpu.CompilerParams(vmem_limit_bytes=24 * 1024 * 1024),
        name="ffn",
    )(place, near_rows, below, above, gate, up, down, first, second)


def local(
    tokens,
    norm_gain,
    expert_ids,
    routing_weight,
    expert_gate,
    expert_up,
    expert_down,
    dense_gate_w,
    dense_up_w,
    dense_down_w,
    dense_gate,
):
    experts = lax.axis_size("ep")
    group_tokens, model_width = tokens.shape
    capacity = 3 * group_tokens // experts
    few = capacity // 2
    rows_mine = experts * few
    part = model_width // (FAR * NEAR)
    wide = model_width // 4
    row_width = model_width // FAR
    hidden_part = expert_gate.shape[2]
    odd_y, odd_x = lax.axis_index("yc"), lax.axis_index("xl")
    mod_y = lax.axis_index("yb") * 2 + odd_y

    gate_t, up_t, down = expert_gate[0].T, expert_up[0].T, expert_down[0]
    split = (hidden_part // 2 + 15) // 16 * 16

    def packed(first, last):
        return jnp.concatenate([w[first:last] for w in (gate_t, up_t, down)], axis=0)

    first_w = send(packed(0, split), lambda y, x: (y, x ^ 1))
    second_w = send(packed(split, hidden_part), lambda y, x: (y, x + (1 if x % 2 else -1)))

    values = tokens.astype(jnp.float32)
    factor = lax.rsqrt(jnp.mean(values * values, axis=-1, keepdims=True) + EPSILON)
    normed = (values * factor * norm_gain[None, :]).astype(jnp.bfloat16)
    ids = expert_ids.T
    shifted = slots_of(ids, experts) - odd_x * few
    places = jnp.where((shifted >= 0) & (shifted < few), ids * few + shifted, -1)
    slot_no = lax.broadcasted_iota(jnp.int32, (rows_mine, group_tokens), 0)
    chosen = [(places[c][None, :] == slot_no).astype(jnp.bfloat16) for c in range(2)]

    def side(weight, other):
        return lax.dynamic_slice_in_dim(weight, (odd_y ^ other) * 2 * wide, 2 * wide, 1)

    outgoing = dot(chosen[0] + chosen[1], side(normed, 0), 1, 0).astype(jnp.bfloat16)
    landed = exchange(outgoing.reshape(experts, few, 2 * wide), "ep")
    landed = landed.reshape(rows_mine, 2 * wide)

    dense_hidden = silu_times(dot(normed, dense_gate_w, 1, 0), dot(normed, dense_up_w, 1, 0))

    def dense_part(step):
        first = (mod_y + step) % 4 * row_width
        down = columns(dense_down_w, [first, first + 4 * row_width], row_width)
        return dot(down, dense_hidden, 0, 1).astype(jnp.bfloat16)

    dense_terms = [
        send(dense_part(1), along_y(1)),
        send(dense_part(2), along_y(2)),
        send(dense_part(3), along_y(-1)),
    ]
    dense_sum = total_of([dense_part(0), *dense_terms])
    dense_sum = dense_sum.reshape(2, NEAR, part, group_tokens)

    def for_x(step):
        there = (lax.axis_index("xh") * 2 + odd_x + step) % NEAR
        return lax.dynamic_index_in_dim(dense_sum, there, 1, keepdims=False)

    dense_x = total_of(
        [for_x(0)] + [send(for_x(k), lambda y, x, k=k: (y, x + k)) for k in range(1, NEAR)]
    )
    high = lax.axis_index("ya")
    dense_mine = lax.dynamic_index_in_dim(dense_x, high, 0, keepdims=False)
    dense_theirs = lax.dynamic_index_in_dim(dense_x, 1 - high, 0, keepdims=False)
    dense_theirs = send(dense_theirs, along_y(4))
    dense_out = dense_mine.astype(jnp.float32) + dense_theirs.astype(jnp.float32)

    arrived = [send(landed[:, :wide], along_y(1)), send(landed[:, wide:], along_y(-1))]

    partial = ffn(odd_y[None], landed, *arrived, gate_t, up_t, down, first_w, second_w)
    near_terms = exchange(partial, ("yc", "xh"))
    near_sum = total_of([near_terms[k] for k in range(4)])
    far_terms = exchange(near_sum, ("ya", "yb"))
    expert_out = total_of([far_terms[k] for k in range(4)])
    returned = exchange(expert_out.reshape(experts, few, 2 * part), "ep")
    returned = returned.reshape(rows_mine, 2 * part)
    weight = routing_weight.T
    routed = sum(weight[c][None, :] * dot(returned, chosen[c], 0, 0) for c in range(2))
    keep = lax.dynamic_slice_in_dim(routed, odd_x * part, part, 0)
    give = lax.dynamic_slice_in_dim(routed, (1 - odd_x) * part, part, 0)
    routed = keep + send(give.astype(jnp.bfloat16), lambda y, x: (y, x ^ 1)).astype(jnp.float32)
    gate_factor = jax.nn.sigmoid(dense_gate)[:, None]
    return (routed + gate_factor * dense_out).astype(jnp.bfloat16).T


def solution(mesh):
    finer = Mesh(mesh.devices.reshape(mesh.shape["ep"], 2, 2, 2, 2, 2), ("ep", *TP))
    in_specs = (
        P("ep", None),
        P(),
        P("ep", None),
        P("ep", None),
        P("ep", None, TP),
        P("ep", None, TP),
        P("ep", TP, None),
        P(None, TP),
        P(None, TP),
        P(TP, None),
        P(TP),
    )
    out_specs = P("ep", TP)
    return jax.shard_map(local, mesh=finer, in_specs=in_specs, out_specs=out_specs, check_vma=False)
```

```python
import jax
import jax.numpy as jnp
from jax import lax
from jax.experimental import pallas as pl
from jax.experimental.pallas import tpu as pltpu
from jax.sharding import Mesh
from jax.sharding import PartitionSpec as P

TP = ("ya", "yb", "yc", "xh", "xl")
FAR, NEAR = 8, 4

EPSILON = 1e-06


def exchange(blocks, axes):
    return lax.all_to_all(blocks, axes, split_axis=0, concat_axis=0, tiled=True)


def send(value, target):
    pairs = []
    for y in range(FAR):
        for x in range(NEAR):
            there_y, there_x = target(y, x)
            pairs.append((y * NEAR + x, there_y % FAR * NEAR + there_x % NEAR))
    return lax.ppermute(value, TP, pairs)


def along_y(steps):
    return lambda y, x: (y + steps, x)


def dot(left, right, left_dim, right_dim):
    return lax.dot_general(
        left, right, (((left_dim,), (right_dim,)), ((), ())), preferred_element_type=jnp.float32
    )


def slots_of(ids, experts):
    tokens = ids.shape[1]
    named = ids[:, None, :] == jnp.arange(experts, dtype=jnp.int32)[None, :, None]
    count = (named[0] | named[1]).astype(jnp.bfloat16)
    before = lax.broadcasted_iota(jnp.int32, (tokens, tokens), 0) < lax.broadcasted_iota(
        jnp.int32, (tokens, tokens), 1
    )
    earlier = dot(count, before.astype(jnp.bfloat16), 1, 0).astype(jnp.int32)
    return jnp.sum(jnp.where(named, earlier[None], 0), axis=1)


def silu_times(gate_act, up_act):
    return (jax.nn.silu(gate_act) * up_act).astype(jnp.bfloat16)


def total_of(terms):
    return sum(term.astype(jnp.float32) for term in terms).astype(jnp.bfloat16)


def columns(weight, starts, size):
    return jnp.concatenate(
        [lax.dynamic_slice_in_dim(weight, start, size, 1) for start in starts], axis=1
    )


def landed_kernel(odd_y, rows, gate, up, first, second, *outs):
    width = rows.shape[1]
    columns_of = pl.ds(pl.multiple_of(odd_y[0] * width, 128), width)
    for ref, out in zip((gate, up, first, second), outs):
        out[...] = dot(ref[pl.ds(0, out.shape[0]), columns_of], rows[...], 1, 1)


def ffn_kernel(
    odd_y, below, above, gate, up, down, first, second, act_0, act_1, act_2, act_3, out
):
    half = below.shape[1]
    beside = (1 - odd_y[0]) * 2 * half
    low = pl.ds(pl.multiple_of(beside, 128), half)
    high = pl.ds(pl.multiple_of(beside + half, 128), half)

    def with_beside(act, ref):
        rows = pl.ds(0, act.shape[0])
        return act[...] + dot(ref[rows, low], below[...], 1, 1) + dot(ref[rows, high], above[...], 1, 1)

    hidden = [silu_times(with_beside(act_0, gate), with_beside(act_1, up))]
    downs = [(down, 0, down.shape[0])]
    for act, ref in ((act_2, first), (act_3, second)):
        count = ref.shape[0] // 3
        both = with_beside(act, ref)
        hidden.append(silu_times(both[:count], both[count:]))
        downs.append((ref, 2 * count, count))
    hidden = jnp.concatenate(hidden, axis=0)
    for q in range(4):
        for y_bit in range(2):
            columns_of = pl.ds((2 * q + y_bit) * 256, 256)
            weights = [ref[pl.ds(start, count), columns_of] for ref, start, count in downs]
            total = dot(hidden, jnp.concatenate(weights, axis=0), 0, 0).astype(jnp.bfloat16)
            for x_bit in range(2):
                out[2 * y_bit + x_bit, q] = total[:, x_bit * 128 : (x_bit + 1) * 128]


def on_core(kernel, flops, moved, out_shape, *operands):
    in_vmem = pl.BlockSpec(memory_space=pltpu.VMEM)
    return pl.pallas_call(
        kernel,
        out_shape=out_shape,
        in_specs=[pl.BlockSpec(memory_space=pltpu.SMEM)] + [in_vmem] * (len(operands) - 1),
        out_specs=jax.tree.map(lambda _: in_vmem, out_shape),
        cost_estimate=pl.CostEstimate(flops=flops, bytes_accessed=moved, transcendentals=0),
        compiler_params=pltpu.CompilerParams(vmem_limit_bytes=24 * 1024 * 1024),
    )(*operands)


def acts_of_landed(odd_y, rows, gate, up, first, second):
    counts = (gate.shape[0], up.shape[0], first.shape[0] // 3 * 2, second.shape[0] // 3 * 2)
    shapes = [jax.ShapeDtypeStruct((count, rows.shape[0]), jnp.float32) for count in counts]
    flops = 2 * rows.size * sum(counts)
    return on_core(
        landed_kernel, flops, 6 * rows.size, shapes, odd_y, rows, gate, up, first, second
    )


def ffn(odd_y, below, above, gate, up, down, first, second, acts):
    rows = below.shape[0]
    units = gate.shape[0] + (first.shape[0] + second.shape[0]) // 3
    shape = jax.ShapeDtypeStruct((4, 4, rows, down.shape[1] // 16), jnp.bfloat16)
    flops = 4 * rows * units * down.shape[1]
    operands = (odd_y, below, above, gate, up, down, first, second, *acts)
    return on_core(ffn_kernel, flops, 6 * units * down.shape[1], shape, *operands)


def local(
    tokens,
    norm_gain,
    expert_ids,
    routing_weight,
    expert_gate,
    expert_up,
    expert_down,
    dense_gate_w,
    dense_up_w,
    dense_down_w,
    dense_gate,
):
    experts = lax.axis_size("ep")
    group_tokens, model_width = tokens.shape
    capacity = 3 * group_tokens // experts
    few = capacity // 2
    rows_mine = experts * few
    part = model_width // (FAR * NEAR)
    wide = model_width // 4
    row_width = model_width // FAR
    hidden_part = expert_gate.shape[2]
    odd_y, odd_x = lax.axis_index("yc"), lax.axis_index("xl")
    mod_y = lax.axis_index("yb") * 2 + odd_y

    gate_t, up_t, down = expert_gate[0].T, expert_up[0].T, expert_down[0]
    split = (hidden_part // 2 + 15) // 16 * 16

    def packed(first, last):
        return jnp.concatenate([w[first:last] for w in (gate_t, up_t, down)], axis=0)

    first_w = send(packed(0, split), lambda y, x: (y, x ^ 1))
    second_w = send(packed(split, hidden_part), lambda y, x: (y, x + (1 if x % 2 else -1)))

    values = tokens.astype(jnp.float32)
    factor = lax.rsqrt(jnp.mean(values * values, axis=-1, keepdims=True) + EPSILON)
    normed = (values * factor * norm_gain[None, :]).astype(jnp.bfloat16)
    ids = expert_ids.T
    shifted = slots_of(ids, experts) - odd_x * few
    places = jnp.where((shifted >= 0) & (shifted < few), ids * few + shifted, -1)
    slot_no = lax.broadcasted_iota(jnp.int32, (rows_mine, group_tokens), 0)
    chosen = [(places[c][None, :] == slot_no).astype(jnp.bfloat16) for c in range(2)]

    def side(weight, other):
        return lax.dynamic_slice_in_dim(weight, (odd_y ^ other) * 2 * wide, 2 * wide, 1)

    outgoing = dot(chosen[0] + chosen[1], side(normed, 0), 1, 0).astype(jnp.bfloat16)
    landed = exchange(outgoing.reshape(experts, few, 2 * wide), "ep")
    landed = landed.reshape(rows_mine, 2 * wide)

    dense_hidden = silu_times(dot(normed, dense_gate_w, 1, 0), dot(normed, dense_up_w, 1, 0))

    def dense_part(step):
        first = (mod_y + step) % 4 * row_width
        down = columns(dense_down_w, [first, first + 4 * row_width], row_width)
        return dot(down, dense_hidden, 0, 1).astype(jnp.bfloat16)

    dense_terms = [
        send(dense_part(1), along_y(1)),
        send(dense_part(2), along_y(2)),
        send(dense_part(3), along_y(-1)),
    ]
    dense_sum = total_of([dense_part(0), *dense_terms])
    dense_sum = dense_sum.reshape(2, NEAR, part, group_tokens)

    def for_x(step):
        there = (lax.axis_index("xh") * 2 + odd_x + step) % NEAR
        return lax.dynamic_index_in_dim(dense_sum, there, 1, keepdims=False)

    dense_x = total_of(
        [for_x(0)] + [send(for_x(k), lambda y, x, k=k: (y, x + k)) for k in range(1, NEAR)]
    )
    high = lax.axis_index("ya")
    dense_mine = lax.dynamic_index_in_dim(dense_x, high, 0, keepdims=False)
    dense_theirs = lax.dynamic_index_in_dim(dense_x, 1 - high, 0, keepdims=False)
    dense_theirs = send(dense_theirs, along_y(4))
    dense_out = dense_mine.astype(jnp.float32) + dense_theirs.astype(jnp.float32)

    arrived = [send(landed[:, :wide], along_y(1)), send(landed[:, wide:], along_y(-1))]

    acts = acts_of_landed(odd_y[None], landed, gate_t, up_t, first_w, second_w)
    partial = ffn(odd_y[None], *arrived, gate_t, up_t, down, first_w, second_w, acts)
    near_terms = exchange(partial, ("yc", "xh"))
    near_sum = total_of([near_terms[k] for k in range(4)])
    far_terms = exchange(near_sum, ("ya", "yb"))
    expert_out = total_of([far_terms[k] for k in range(4)])
    returned = exchange(expert_out.reshape(experts, few, 2 * part), "ep")
    returned = returned.reshape(rows_mine, 2 * part)
    weight = routing_weight.T
    routed = sum(weight[c][None, :] * dot(returned, chosen[c], 0, 0) for c in range(2))
    keep = lax.dynamic_slice_in_dim(routed, odd_x * part, part, 0)
    give = lax.dynamic_slice_in_dim(routed, (1 - odd_x) * part, part, 0)
    routed = keep + send(give.astype(jnp.bfloat16), lambda y, x: (y, x ^ 1)).astype(jnp.float32)
    gate_factor = jax.nn.sigmoid(dense_gate)[:, None]
    return (routed + gate_factor * dense_out).astype(jnp.bfloat16).T


def solution(mesh):
    finer = Mesh(mesh.devices.reshape(mesh.shape["ep"], 2, 2, 2, 2, 2), ("ep", *TP))
    in_specs = (
        P("ep", None),
        P(),
        P("ep", None),
        P("ep", None),
        P("ep", None, TP),
        P("ep", None, TP),
        P("ep", TP, None),
        P(None, TP),
        P(None, TP),
        P(TP, None),
        P(TP),
    )
    out_specs = P("ep", TP)
    return jax.shard_map(local, mesh=finer, in_specs=in_specs, out_specs=out_specs, check_vma=False)
```

```python
import jax
import jax.numpy as jnp
from jax import lax
from jax.experimental import pallas as pl
from jax.experimental.pallas import tpu as pltpu
from jax.sharding import Mesh
from jax.sharding import PartitionSpec as P

TP = ("ya", "yb", "yc", "xh", "xl")
FAR, NEAR = 8, 4

EPSILON = 1e-06


def exchange(blocks, axes):
    return lax.all_to_all(blocks, axes, split_axis=0, concat_axis=0, tiled=True)


def send(value, target):
    pairs = []
    for y in range(FAR):
        for x in range(NEAR):
            there_y, there_x = target(y, x)
            pairs.append((y * NEAR + x, there_y % FAR * NEAR + there_x % NEAR))
    return lax.ppermute(value, TP, pairs)


def along_y(steps):
    return lambda y, x: (y + steps, x)


def dot(left, right, left_dim, right_dim):
    return lax.dot_general(
        left, right, (((left_dim,), (right_dim,)), ((), ())), preferred_element_type=jnp.float32
    )


def slots_of(ids, experts):
    tokens = ids.shape[1]
    named = ids[:, None, :] == jnp.arange(experts, dtype=jnp.int32)[None, :, None]
    count = (named[0] | named[1]).astype(jnp.bfloat16)
    before = lax.broadcasted_iota(jnp.int32, (tokens, tokens), 0) < lax.broadcasted_iota(
        jnp.int32, (tokens, tokens), 1
    )
    earlier = dot(count, before.astype(jnp.bfloat16), 1, 0).astype(jnp.int32)
    return jnp.sum(jnp.where(named, earlier[None], 0), axis=1)


def silu_times(gate_act, up_act):
    return (jax.nn.silu(gate_act) * up_act).astype(jnp.bfloat16)


def total_of(terms):
    return sum(term.astype(jnp.float32) for term in terms).astype(jnp.bfloat16)


def columns(weight, starts, size):
    return jnp.concatenate(
        [lax.dynamic_slice_in_dim(weight, start, size, 1) for start in starts], axis=1
    )


def landed_kernel(odd_y, rows, gate, up, first, second, *outs):
    width = rows.shape[1]
    columns_of = pl.ds(pl.multiple_of(odd_y[0] * width, 128), width)
    for ref, out in zip((gate, up, first, second), outs):
        out[...] = dot(ref[pl.ds(0, out.shape[0]), columns_of], rows[...], 1, 1)


def ffn_kernel(
    odd_y, below, above, gate, up, down, first, second, act_0, act_1, act_2, act_3, out
):
    half = below.shape[1]
    beside = (1 - odd_y[0]) * 2 * half
    low = pl.ds(pl.multiple_of(beside, 128), half)
    high = pl.ds(pl.multiple_of(beside + half, 128), half)

    def with_beside(act, ref):
        rows = pl.ds(0, act.shape[0])
        return act[...] + dot(ref[rows, low], below[...], 1, 1) + dot(ref[rows, high], above[...], 1, 1)

    hidden = [silu_times(with_beside(act_0, gate), with_beside(act_1, up))]
    downs = [(down, 0, down.shape[0])]
    for act, ref in ((act_2, first), (act_3, second)):
        count = ref.shape[0] // 3
        both = with_beside(act, ref)
        hidden.append(silu_times(both[:count], both[count:]))
        downs.append((ref, 2 * count, count))
    hidden = jnp.concatenate(hidden, axis=0)
    for q in range(4):
        for y_bit in range(2):
            columns_of = pl.ds((2 * q + y_bit) * 256, 256)
            weights = [ref[pl.ds(start, count), columns_of] for ref, start, count in downs]
            total = dot(hidden, jnp.concatenate(weights, axis=0), 0, 0).astype(jnp.bfloat16)
            for x_bit in range(2):
                piece = total[:, x_bit * 128 : (x_bit + 1) * 128]
                out[2 * y_bit + x_bit, :, q * 128 : (q + 1) * 128] = piece


def on_core(kernel, flops, moved, out_shape, *operands):
    in_vmem = pl.BlockSpec(memory_space=pltpu.VMEM)
    return pl.pallas_call(
        kernel,
        out_shape=out_shape,
        in_specs=[pl.BlockSpec(memory_space=pltpu.SMEM)] + [in_vmem] * (len(operands) - 1),
        out_specs=jax.tree.map(lambda _: in_vmem, out_shape),
        cost_estimate=pl.CostEstimate(flops=flops, bytes_accessed=moved, transcendentals=0),
        compiler_params=pltpu.CompilerParams(vmem_limit_bytes=24 * 1024 * 1024),
    )(*operands)


def acts_of_landed(odd_y, rows, gate, up, first, second):
    counts = (gate.shape[0], up.shape[0], first.shape[0] // 3 * 2, second.shape[0] // 3 * 2)
    shapes = [jax.ShapeDtypeStruct((count, rows.shape[0]), jnp.float32) for count in counts]
    flops = 2 * rows.size * sum(counts)
    return on_core(
        landed_kernel, flops, 6 * rows.size, shapes, odd_y, rows, gate, up, first, second
    )


def ffn(odd_y, below, above, gate, up, down, first, second, acts):
    rows = below.shape[0]
    units = gate.shape[0] + (first.shape[0] + second.shape[0]) // 3
    shape = jax.ShapeDtypeStruct((4, rows, down.shape[1] // 4), jnp.bfloat16)
    flops = 4 * rows * units * down.shape[1]
    operands = (odd_y, below, above, gate, up, down, first, second, *acts)
    return on_core(ffn_kernel, flops, 6 * units * down.shape[1], shape, *operands)


def local(
    tokens,
    norm_gain,
    expert_ids,
    routing_weight,
    expert_gate,
    expert_up,
    expert_down,
    dense_gate_w,
    dense_up_w,
    dense_down_w,
    dense_gate,
):
    experts = lax.axis_size("ep")
    group_tokens, model_width = tokens.shape
    capacity = 3 * group_tokens // experts
    few = capacity // 2
    rows_mine = experts * few
    part = model_width // (FAR * NEAR)
    wide = model_width // 4
    row_width = model_width // FAR
    hidden_part = expert_gate.shape[2]
    odd_y, odd_x = lax.axis_index("yc"), lax.axis_index("xl")
    mod_y = lax.axis_index("yb") * 2 + odd_y

    gate_t, up_t, down = expert_gate[0].T, expert_up[0].T, expert_down[0]
    split = (hidden_part // 2 + 15) // 16 * 16

    def packed(first, last):
        return jnp.concatenate([w[first:last] for w in (gate_t, up_t, down)], axis=0)

    first_w = send(packed(0, split), lambda y, x: (y, x ^ 1))
    second_w = send(packed(split, hidden_part), lambda y, x: (y, x + (1 if x % 2 else -1)))

    values = tokens.astype(jnp.float32)
    factor = lax.rsqrt(jnp.mean(values * values, axis=-1, keepdims=True) + EPSILON)
    normed = (values * factor * norm_gain[None, :]).astype(jnp.bfloat16)
    ids = expert_ids.T
    shifted = slots_of(ids, experts) - odd_x * few
    places = jnp.where((shifted >= 0) & (shifted < few), ids * few + shifted, -1)
    slot_no = lax.broadcasted_iota(jnp.int32, (rows_mine, group_tokens), 0)
    chosen = [(places[c][None, :] == slot_no).astype(jnp.bfloat16) for c in range(2)]

    def side(weight, other):
        return lax.dynamic_slice_in_dim(weight, (odd_y ^ other) * 2 * wide, 2 * wide, 1)

    outgoing = dot(chosen[0] + chosen[1], side(normed, 0), 1, 0).astype(jnp.bfloat16)
    landed = exchange(outgoing.reshape(experts, few, 2 * wide), "ep")
    landed = landed.reshape(rows_mine, 2 * wide)

    dense_hidden = silu_times(dot(normed, dense_gate_w, 1, 0), dot(normed, dense_up_w, 1, 0))

    def dense_part(step):
        first = (mod_y + step) % 4 * row_width
        down = columns(dense_down_w, [first, first + 4 * row_width], row_width)
        return dot(down, dense_hidden, 0, 1).astype(jnp.bfloat16)

    dense_terms = [
        send(dense_part(1), along_y(1)),
        send(dense_part(2), along_y(2)),
        send(dense_part(3), along_y(-1)),
    ]
    dense_sum = total_of([dense_part(0), *dense_terms])
    dense_sum = dense_sum.reshape(2, NEAR, part, group_tokens)

    def for_x(step):
        there = (lax.axis_index("xh") * 2 + odd_x + step) % NEAR
        return lax.dynamic_index_in_dim(dense_sum, there, 1, keepdims=False)

    dense_x = total_of(
        [for_x(0)] + [send(for_x(k), lambda y, x, k=k: (y, x + k)) for k in range(1, NEAR)]
    )
    high = lax.axis_index("ya")
    dense_mine = lax.dynamic_index_in_dim(dense_x, high, 0, keepdims=False)
    dense_theirs = lax.dynamic_index_in_dim(dense_x, 1 - high, 0, keepdims=False)
    dense_theirs = send(dense_theirs, along_y(4))
    dense_out = dense_mine.astype(jnp.float32) + dense_theirs.astype(jnp.float32)

    arrived = [
        send(landed[:, :wide], lambda y, x: (y ^ 1, x)),
        send(landed[:, wide:], lambda y, x: (y + (1 if y % 2 else -1), x)),
    ]

    acts = acts_of_landed(odd_y[None], landed, gate_t, up_t, first_w, second_w)
    partial = ffn(odd_y[None], *arrived, gate_t, up_t, down, first_w, second_w, acts)
    near_terms = exchange(partial, ("yc", "xh"))
    near_sum = total_of([near_terms[k] for k in range(4)])
    returned = exchange(near_sum.reshape(experts, few, wide), "ep")
    returned = returned.reshape(rows_mine, wide)
    weight = routing_weight.T
    routed = sum(weight[c][None, :] * dot(returned, chosen[c], 0, 0) for c in range(2))
    pieces = exchange(
        routed.astype(jnp.bfloat16).reshape(8, part, group_tokens), ("ya", "yb", "xl")
    )
    routed = pieces.astype(jnp.float32).sum(axis=0)
    gate_factor = jax.nn.sigmoid(dense_gate)[:, None]
    return (routed + gate_factor * dense_out).astype(jnp.bfloat16).T


def solution(mesh):
    finer = Mesh(mesh.devices.reshape(mesh.shape["ep"], 2, 2, 2, 2, 2), ("ep", *TP))
    in_specs = (
        P("ep", None),
        P(),
        P("ep", None),
        P("ep", None),
        P("ep", None, TP),
        P("ep", None, TP),
        P("ep", TP, None),
        P(None, TP),
        P(None, TP),
        P(TP, None),
        P(TP),
    )
    out_specs = P("ep", TP)
    return jax.shard_map(local, mesh=finer, in_specs=in_specs, out_specs=out_specs, check_vma=False)
```

```python
import jax
import jax.numpy as jnp
from jax import lax
from jax.experimental import pallas as pl
from jax.experimental.pallas import tpu as pltpu
from jax.sharding import Mesh
from jax.sharding import PartitionSpec as P

TP = ("ya", "yb", "yc", "xh", "xl")
FAR, NEAR = 8, 4

EPSILON = 1e-06


def exchange(blocks, axes):
    return lax.all_to_all(blocks, axes, split_axis=0, concat_axis=0, tiled=True)


def send(value, target):
    pairs = []
    for y in range(FAR):
        for x in range(NEAR):
            there_y, there_x = target(y, x)
            pairs.append((y * NEAR + x, there_y % FAR * NEAR + there_x % NEAR))
    return lax.ppermute(value, TP, pairs)


def along_y(steps):
    return lambda y, x: (y + steps, x)


def dot(left, right, left_dim, right_dim):
    return lax.dot_general(
        left, right, (((left_dim,), (right_dim,)), ((), ())), preferred_element_type=jnp.float32
    )


def silu_times(gate_act, up_act):
    return (jax.nn.silu(gate_act) * up_act).astype(jnp.bfloat16)


def total_of(terms):
    return sum(term.astype(jnp.float32) for term in terms).astype(jnp.bfloat16)


def columns(weight, starts, size):
    return jnp.concatenate(
        [lax.dynamic_slice_in_dim(weight, start, size, 1) for start in starts], axis=1
    )


def front_kernel(where, ids, tokens, gain, rows, factors, places):
    experts = 32
    count, width = tokens.shape[0], rows.shape[1]
    few = rows.shape[0] // 24
    values = tokens[...].astype(jnp.float32)
    factor = lax.rsqrt(jnp.mean(values * values, axis=-1, keepdims=True) + EPSILON)
    factors[...] = factor
    mine = pl.ds(pl.multiple_of(where[0] * width, 128), width)
    normed = (tokens[:, mine].astype(jnp.float32) * factor * gain[:, mine]).astype(jnp.bfloat16)
    expert_no = lax.broadcasted_iota(jnp.int32, (experts, count), 0)
    named = [ids[c : c + 1, :] == expert_no for c in range(2)]
    ones = jnp.where(named[0] | named[1], 1.0, 0.0).astype(jnp.bfloat16)
    from_token = lax.broadcasted_iota(jnp.int32, (count, count), 0)
    to_token = lax.broadcasted_iota(jnp.int32, (count, count), 1)
    before = jnp.where(from_token < to_token, 1.0, 0.0).astype(jnp.bfloat16)
    earlier = dot(ones, before, 1, 0)
    slot_no = lax.broadcasted_iota(jnp.int32, (rows.shape[0], count), 0)
    hits = None
    for c in range(2):
        slot = jnp.sum(jnp.where(named[c], earlier, 0.0), axis=0, keepdims=True)
        shifted = slot.astype(jnp.int32) - where[1] * few
        place = jnp.where((shifted >= 0) & (shifted < few), ids[c : c + 1, :] * few + shifted, -1)
        places[c : c + 1, :] = place
        hit = place == slot_no
        hits = hit if hits is None else hits | hit
    chosen = jnp.where(hits, 1.0, 0.0).astype(jnp.bfloat16)
    rows[...] = dot(chosen, normed, 1, 0).astype(jnp.bfloat16)


def landed_kernel(odd_y, rows, gate, up, first, second, *outs):
    width = rows.shape[1]
    columns_of = pl.ds(pl.multiple_of(odd_y[0] * width, 128), width)
    for ref, out in zip((gate, up, first, second), outs):
        out[...] = dot(ref[pl.ds(0, out.shape[0]), columns_of], rows[...], 1, 1)


def ffn_kernel(
    odd_y, below, above, gate, up, down, first, second, act_0, act_1, act_2, act_3, out
):
    half = below.shape[1]
    beside = (1 - odd_y[0]) * 2 * half
    low = pl.ds(pl.multiple_of(beside, 128), half)
    high = pl.ds(pl.multiple_of(beside + half, 128), half)

    def with_beside(act, ref):
        rows = pl.ds(0, act.shape[0])
        return act[...] + dot(ref[rows, low], below[...], 1, 1) + dot(ref[rows, high], above[...], 1, 1)

    hidden = [silu_times(with_beside(act_0, gate), with_beside(act_1, up))]
    downs = [(down, 0, down.shape[0])]
    for act, ref in ((act_2, first), (act_3, second)):
        count = ref.shape[0] // 3
        both = with_beside(act, ref)
        hidden.append(silu_times(both[:count], both[count:]))
        downs.append((ref, 2 * count, count))
    hidden = jnp.concatenate(hidden, axis=0)
    for q in range(4):
        for y_bit in range(2):
            columns_of = pl.ds((2 * q + y_bit) * 256, 256)
            weights = [ref[pl.ds(start, count), columns_of] for ref, start, count in downs]
            total = dot(hidden, jnp.concatenate(weights, axis=0), 0, 0).astype(jnp.bfloat16)
            for x_bit in range(2):
                piece = total[:, x_bit * 128 : (x_bit + 1) * 128]
                out[2 * y_bit + x_bit, :, q * 128 : (q + 1) * 128] = piece


def on_core(kernel, flops, moved, out_shape, *operands):
    in_vmem = pl.BlockSpec(memory_space=pltpu.VMEM)
    return pl.pallas_call(
        kernel,
        out_shape=out_shape,
        in_specs=[pl.BlockSpec(memory_space=pltpu.SMEM)] + [in_vmem] * (len(operands) - 1),
        out_specs=jax.tree.map(lambda _: in_vmem, out_shape),
        cost_estimate=pl.CostEstimate(flops=flops, bytes_accessed=moved, transcendentals=0),
        compiler_params=pltpu.CompilerParams(vmem_limit_bytes=24 * 1024 * 1024),
    )(*operands)


def front(where, ids, tokens, gain, rows, width):
    count = tokens.shape[0]
    shapes = [
        jax.ShapeDtypeStruct((rows, width), jnp.bfloat16),
        jax.ShapeDtypeStruct((count, 1), jnp.float32),
        jax.ShapeDtypeStruct((2, count), jnp.int32),
    ]
    flops = 2 * rows * count * width
    return on_core(front_kernel, flops, 2 * tokens.size, shapes, where, ids, tokens, gain)


def acts_of_landed(odd_y, rows, gate, up, first, second):
    counts = (gate.shape[0], up.shape[0], first.shape[0] // 3 * 2, second.shape[0] // 3 * 2)
    shapes = [jax.ShapeDtypeStruct((count, rows.shape[0]), jnp.float32) for count in counts]
    flops = 2 * rows.size * sum(counts)
    return on_core(
        landed_kernel, flops, 6 * rows.size, shapes, odd_y, rows, gate, up, first, second
    )


def ffn(odd_y, below, above, gate, up, down, first, second, acts):
    rows = below.shape[0]
    units = gate.shape[0] + (first.shape[0] + second.shape[0]) // 3
    shape = jax.ShapeDtypeStruct((4, rows, down.shape[1] // 4), jnp.bfloat16)
    flops = 4 * rows * units * down.shape[1]
    operands = (odd_y, below, above, gate, up, down, first, second, *acts)
    return on_core(ffn_kernel, flops, 6 * units * down.shape[1], shape, *operands)


def local(
    tokens,
    norm_gain,
    expert_ids,
    routing_weight,
    expert_gate,
    expert_up,
    expert_down,
    dense_gate_w,
    dense_up_w,
    dense_down_w,
    dense_gate,
):
    experts = lax.axis_size("ep")
    group_tokens, model_width = tokens.shape
    capacity = 3 * group_tokens // experts
    few = capacity // 2
    rows_mine = experts * few
    part = model_width // (FAR * NEAR)
    wide = model_width // 4
    row_width = model_width // FAR
    hidden_part = expert_gate.shape[2]
    odd_y, odd_x = lax.axis_index("yc"), lax.axis_index("xl")
    mod_y = lax.axis_index("yb") * 2 + odd_y

    gate_t, up_t, down = expert_gate[0].T, expert_up[0].T, expert_down[0]
    split = (hidden_part // 2 + 15) // 16 * 16

    def packed(first, last):
        return jnp.concatenate([w[first:last] for w in (gate_t, up_t, down)], axis=0)

    first_w = send(packed(0, split), lambda y, x: (y, x ^ 1))
    second_w = send(packed(split, hidden_part), lambda y, x: (y, x + (1 if x % 2 else -1)))

    where = jnp.stack([odd_y, odd_x])
    outgoing, factor, places = front(
        where, expert_ids.T, tokens, norm_gain[None, :], rows_mine, 2 * wide
    )
    normed = (tokens.astype(jnp.float32) * factor * norm_gain[None, :]).astype(jnp.bfloat16)
    slot_no = lax.broadcasted_iota(jnp.int32, (rows_mine, group_tokens), 0)
    chosen = [(places[c][None, :] == slot_no).astype(jnp.bfloat16) for c in range(2)]
    landed = exchange(outgoing.reshape(experts, few, 2 * wide), "ep")
    landed = landed.reshape(rows_mine, 2 * wide)

    dense_hidden = silu_times(dot(normed, dense_gate_w, 1, 0), dot(normed, dense_up_w, 1, 0))

    def dense_part(step):
        first = (mod_y + step) % 4 * row_width
        down = columns(dense_down_w, [first, first + 4 * row_width], row_width)
        return dot(down, dense_hidden, 0, 1).astype(jnp.bfloat16)

    dense_terms = [
        send(dense_part(1), along_y(1)),
        send(dense_part(2), along_y(2)),
        send(dense_part(3), along_y(-1)),
    ]
    dense_sum = total_of([dense_part(0), *dense_terms])
    dense_sum = dense_sum.reshape(2, NEAR, part, group_tokens)

    def for_x(step):
        there = (lax.axis_index("xh") * 2 + odd_x + step) % NEAR
        return lax.dynamic_index_in_dim(dense_sum, there, 1, keepdims=False)

    dense_x = total_of(
        [for_x(0)] + [send(for_x(k), lambda y, x, k=k: (y, x + k)) for k in range(1, NEAR)]
    )
    high = lax.axis_index("ya")
    dense_mine = lax.dynamic_index_in_dim(dense_x, high, 0, keepdims=False)
    dense_theirs = lax.dynamic_index_in_dim(dense_x, 1 - high, 0, keepdims=False)
    dense_theirs = send(dense_theirs, along_y(4))
    dense_out = dense_mine.astype(jnp.float32) + dense_theirs.astype(jnp.float32)

    arrived = [
        send(landed[:, :wide], lambda y, x: (y ^ 1, x)),
        send(landed[:, wide:], lambda y, x: (y + (1 if y % 2 else -1), x)),
    ]

    acts = acts_of_landed(odd_y[None], landed, gate_t, up_t, first_w, second_w)
    partial = ffn(odd_y[None], *arrived, gate_t, up_t, down, first_w, second_w, acts)
    near_terms = exchange(partial, ("yc", "xh"))
    near_sum = total_of([near_terms[k] for k in range(4)])
    returned = exchange(near_sum.reshape(experts, few, wide), "ep")
    returned = returned.reshape(rows_mine, wide)
    weight = routing_weight.T
    routed = sum(weight[c][None, :] * dot(returned, chosen[c], 0, 0) for c in range(2))
    pieces = exchange(
        routed.astype(jnp.bfloat16).reshape(8, part, group_tokens), ("ya", "yb", "xl")
    )
    routed = pieces.astype(jnp.float32).sum(axis=0)
    gate_factor = jax.nn.sigmoid(dense_gate)[:, None]
    return (routed + gate_factor * dense_out).astype(jnp.bfloat16).T


def solution(mesh):
    finer = Mesh(mesh.devices.reshape(mesh.shape["ep"], 2, 2, 2, 2, 2), ("ep", *TP))
    in_specs = (
        P("ep", None),
        P(),
        P("ep", None),
        P("ep", None),
        P("ep", None, TP),
        P("ep", None, TP),
        P("ep", TP, None),
        P(None, TP),
        P(None, TP),
        P(TP, None),
        P(TP),
    )
    out_specs = P("ep", TP)
    return jax.shard_map(local, mesh=finer, in_specs=in_specs, out_specs=out_specs, check_vma=False)
```

```python
import jax
import jax.numpy as jnp
from jax import lax
from jax.experimental import pallas as pl
from jax.experimental.pallas import tpu as pltpu
from jax.sharding import Mesh
from jax.sharding import PartitionSpec as P

TP = ("ya", "yb", "yc", "xh", "xl")
FAR, NEAR = 8, 4

EPSILON = 1e-06


def exchange(blocks, axes):
    return lax.all_to_all(blocks, axes, split_axis=0, concat_axis=0, tiled=True)


def send(value, target):
    pairs = []
    for y in range(FAR):
        for x in range(NEAR):
            there_y, there_x = target(y, x)
            pairs.append((y * NEAR + x, there_y % FAR * NEAR + there_x % NEAR))
    return lax.ppermute(value, TP, pairs)


def along_y(steps):
    return lambda y, x: (y + steps, x)


def dot(left, right, left_dim, right_dim):
    return lax.dot_general(
        left, right, (((left_dim,), (right_dim,)), ((), ())), preferred_element_type=jnp.float32
    )


def silu_times(gate_act, up_act):
    return (jax.nn.silu(gate_act) * up_act).astype(jnp.bfloat16)


def total_of(terms):
    return sum(term.astype(jnp.float32) for term in terms).astype(jnp.bfloat16)


def columns(weight, starts, size):
    return jnp.concatenate(
        [lax.dynamic_slice_in_dim(weight, start, size, 1) for start in starts], axis=1
    )


def front_kernel(where, ids, tokens, gain, gate, up, rows, dense_hidden, places):
    experts = 32
    count, width = tokens.shape[0], rows.shape[1]
    few = rows.shape[0] // 24
    values = tokens[...].astype(jnp.float32)
    factor = lax.rsqrt(jnp.mean(values * values, axis=-1, keepdims=True) + EPSILON)
    whole = (values * factor * gain[...]).astype(jnp.bfloat16)
    dense_hidden[...] = silu_times(dot(whole, gate[...], 1, 1), dot(whole, up[...], 1, 1))
    mine = pl.ds(pl.multiple_of(where[0] * width, 128), width)
    normed = (tokens[:, mine].astype(jnp.float32) * factor * gain[:, mine]).astype(jnp.bfloat16)
    expert_no = lax.broadcasted_iota(jnp.int32, (experts, count), 0)
    named = [ids[c : c + 1, :] == expert_no for c in range(2)]
    ones = jnp.where(named[0] | named[1], 1.0, 0.0).astype(jnp.bfloat16)
    from_token = lax.broadcasted_iota(jnp.int32, (count, count), 0)
    to_token = lax.broadcasted_iota(jnp.int32, (count, count), 1)
    before = jnp.where(from_token < to_token, 1.0, 0.0).astype(jnp.bfloat16)
    earlier = dot(ones, before, 1, 0)
    slot_no = lax.broadcasted_iota(jnp.int32, (rows.shape[0], count), 0)
    hits = None
    for c in range(2):
        slot = jnp.sum(jnp.where(named[c], earlier, 0.0), axis=0, keepdims=True)
        shifted = slot.astype(jnp.int32) - where[1] * few
        place = jnp.where((shifted >= 0) & (shifted < few), ids[c : c + 1, :] * few + shifted, -1)
        places[c : c + 1, :] = place
        hit = place == slot_no
        hits = hit if hits is None else hits | hit
    chosen = jnp.where(hits, 1.0, 0.0).astype(jnp.bfloat16)
    rows[...] = dot(chosen, normed, 1, 0).astype(jnp.bfloat16)


def landed_kernel(odd_y, rows, gate, up, first, second, *outs):
    width = rows.shape[1]
    columns_of = pl.ds(pl.multiple_of(odd_y[0] * width, 128), width)
    for ref, out in zip((gate, up, first, second), outs):
        out[...] = dot(ref[pl.ds(0, out.shape[0]), columns_of], rows[...], 1, 1)


def ffn_kernel(
    odd_y, below, above, gate, up, down, first, second, act_0, act_1, act_2, act_3, out
):
    half = below.shape[1]
    beside = (1 - odd_y[0]) * 2 * half
    low = pl.ds(pl.multiple_of(beside, 128), half)
    high = pl.ds(pl.multiple_of(beside + half, 128), half)

    def with_beside(act, ref):
        rows = pl.ds(0, act.shape[0])
        return act[...] + dot(ref[rows, low], below[...], 1, 1) + dot(ref[rows, high], above[...], 1, 1)

    hidden = [silu_times(with_beside(act_0, gate), with_beside(act_1, up))]
    downs = [(down, 0, down.shape[0])]
    for act, ref in ((act_2, first), (act_3, second)):
        count = ref.shape[0] // 3
        both = with_beside(act, ref)
        hidden.append(silu_times(both[:count], both[count:]))
        downs.append((ref, 2 * count, count))
    hidden = jnp.concatenate(hidden, axis=0)
    for q in range(4):
        for y_bit in range(2):
            columns_of = pl.ds((2 * q + y_bit) * 256, 256)
            weights = [ref[pl.ds(start, count), columns_of] for ref, start, count in downs]
            total = dot(hidden, jnp.concatenate(weights, axis=0), 0, 0).astype(jnp.bfloat16)
            for x_bit in range(2):
                piece = total[:, x_bit * 128 : (x_bit + 1) * 128]
                out[2 * y_bit + x_bit, :, q * 128 : (q + 1) * 128] = piece


def on_core(kernel, flops, moved, out_shape, *operands):
    in_vmem = pl.BlockSpec(memory_space=pltpu.VMEM)
    return pl.pallas_call(
        kernel,
        out_shape=out_shape,
        in_specs=[pl.BlockSpec(memory_space=pltpu.SMEM)] + [in_vmem] * (len(operands) - 1),
        out_specs=jax.tree.map(lambda _: in_vmem, out_shape),
        cost_estimate=pl.CostEstimate(flops=flops, bytes_accessed=moved, transcendentals=0),
        compiler_params=pltpu.CompilerParams(vmem_limit_bytes=24 * 1024 * 1024),
    )(*operands)


def front(where, ids, tokens, gain, gate, up, rows, width):
    count = tokens.shape[0]
    shapes = [
        jax.ShapeDtypeStruct((rows, width), jnp.bfloat16),
        jax.ShapeDtypeStruct((count, gate.shape[0]), jnp.bfloat16),
        jax.ShapeDtypeStruct((2, count), jnp.int32),
    ]
    flops = 2 * rows * count * width
    operands = (where, ids, tokens, gain, gate, up)
    return on_core(front_kernel, flops, 2 * tokens.size, shapes, *operands)


def acts_of_landed(odd_y, rows, gate, up, first, second):
    counts = (gate.shape[0], up.shape[0], first.shape[0] // 3 * 2, second.shape[0] // 3 * 2)
    shapes = [jax.ShapeDtypeStruct((count, rows.shape[0]), jnp.float32) for count in counts]
    flops = 2 * rows.size * sum(counts)
    return on_core(
        landed_kernel, flops, 6 * rows.size, shapes, odd_y, rows, gate, up, first, second
    )


def ffn(odd_y, below, above, gate, up, down, first, second, acts):
    rows = below.shape[0]
    units = gate.shape[0] + (first.shape[0] + second.shape[0]) // 3
    shape = jax.ShapeDtypeStruct((4, rows, down.shape[1] // 4), jnp.bfloat16)
    flops = 4 * rows * units * down.shape[1]
    operands = (odd_y, below, above, gate, up, down, first, second, *acts)
    return on_core(ffn_kernel, flops, 6 * units * down.shape[1], shape, *operands)


def local(
    tokens,
    norm_gain,
    expert_ids,
    routing_weight,
    expert_gate,
    expert_up,
    expert_down,
    dense_gate_w,
    dense_up_w,
    dense_down_w,
    dense_gate,
):
    experts = lax.axis_size("ep")
    group_tokens, model_width = tokens.shape
    capacity = 3 * group_tokens // experts
    few = capacity // 2
    rows_mine = experts * few
    part = model_width // (FAR * NEAR)
    wide = model_width // 4
    row_width = model_width // FAR
    hidden_part = expert_gate.shape[2]
    odd_y, odd_x = lax.axis_index("yc"), lax.axis_index("xl")
    mod_y = lax.axis_index("yb") * 2 + odd_y

    gate_t, up_t, down = expert_gate[0].T, expert_up[0].T, expert_down[0]
    split = (hidden_part // 2 + 15) // 16 * 16

    def packed(first, last):
        return jnp.concatenate([w[first:last] for w in (gate_t, up_t, down)], axis=0)

    first_w = send(packed(0, split), lambda y, x: (y, x ^ 1))
    second_w = send(packed(split, hidden_part), lambda y, x: (y, x + (1 if x % 2 else -1)))

    where = jnp.stack([odd_y, odd_x])
    outgoing, dense_hidden, places = front(
        where,
        expert_ids.T,
        tokens,
        norm_gain[None, :],
        dense_gate_w.T,
        dense_up_w.T,
        rows_mine,
        2 * wide,
    )
    slot_no = lax.broadcasted_iota(jnp.int32, (rows_mine, group_tokens), 0)
    chosen = [(places[c][None, :] == slot_no).astype(jnp.bfloat16) for c in range(2)]
    landed = exchange(outgoing.reshape(experts, few, 2 * wide), "ep")
    landed = landed.reshape(rows_mine, 2 * wide)


    def dense_part(step):
        first = (mod_y + step) % 4 * row_width
        down = columns(dense_down_w, [first, first + 4 * row_width], row_width)
        return dot(down, dense_hidden, 0, 1).astype(jnp.bfloat16)

    dense_terms = [
        send(dense_part(1), along_y(1)),
        send(dense_part(2), along_y(2)),
        send(dense_part(3), along_y(-1)),
    ]
    dense_sum = total_of([dense_part(0), *dense_terms])
    dense_sum = dense_sum.reshape(2, NEAR, part, group_tokens)

    def for_x(step):
        there = (lax.axis_index("xh") * 2 + odd_x + step) % NEAR
        return lax.dynamic_index_in_dim(dense_sum, there, 1, keepdims=False)

    dense_x = total_of(
        [for_x(0)] + [send(for_x(k), lambda y, x, k=k: (y, x + k)) for k in range(1, NEAR)]
    )
    high = lax.axis_index("ya")
    dense_mine = lax.dynamic_index_in_dim(dense_x, high, 0, keepdims=False)
    dense_theirs = lax.dynamic_index_in_dim(dense_x, 1 - high, 0, keepdims=False)
    dense_theirs = send(dense_theirs, along_y(4))
    dense_out = dense_mine.astype(jnp.float32) + dense_theirs.astype(jnp.float32)

    arrived = [
        send(landed[:, :wide], lambda y, x: (y ^ 1, x)),
        send(landed[:, wide:], lambda y, x: (y + (1 if y % 2 else -1), x)),
    ]

    acts = acts_of_landed(odd_y[None], landed, gate_t, up_t, first_w, second_w)
    partial = ffn(odd_y[None], *arrived, gate_t, up_t, down, first_w, second_w, acts)
    near_terms = exchange(partial, ("yc", "xh"))
    near_sum = total_of([near_terms[k] for k in range(4)])
    returned = exchange(near_sum.reshape(experts, few, wide), "ep")
    returned = returned.reshape(rows_mine, wide)
    weight = routing_weight.T
    routed = sum(weight[c][None, :] * dot(returned, chosen[c], 0, 0) for c in range(2))
    pieces = exchange(
        routed.astype(jnp.bfloat16).reshape(8, part, group_tokens), ("ya", "yb", "xl")
    )
    routed = pieces.astype(jnp.float32).sum(axis=0)
    gate_factor = jax.nn.sigmoid(dense_gate)[:, None]
    return (routed + gate_factor * dense_out).astype(jnp.bfloat16).T


def solution(mesh):
    finer = Mesh(mesh.devices.reshape(mesh.shape["ep"], 2, 2, 2, 2, 2), ("ep", *TP))
    in_specs = (
        P("ep", None),
        P(),
        P("ep", None),
        P("ep", None),
        P("ep", None, TP),
        P("ep", None, TP),
        P("ep", TP, None),
        P(None, TP),
        P(None, TP),
        P(TP, None),
        P(TP),
    )
    out_specs = P("ep", TP)
    return jax.shard_map(local, mesh=finer, in_specs=in_specs, out_specs=out_specs, check_vma=False)
```
